128 devices in a mesh: sp: 16 (over z, x), tp: 8 (over y, core).
Axes of the slice: x: 4, y: 4, z: 4, core: 2. Of those that a mesh axis runs over, the one named last changes fastest.
Arguments:
- tokens: bfloat16 [16384, 2048], P('sp', 'tp'), may hold values from -16 to 16
- norm_gain: float32 [2048], replicated, may hold values from 0.1 to 1.9
- signal_proj: bfloat16 [2048, 1024], P(None, 'tp'), may hold values from -0.125 to 0.125
- postgate_proj: bfloat16 [2048, 1024], P(None, 'tp'), may hold values from -0.125 to 0.125
- pregate_proj: bfloat16 [2048, 1024], P(None, 'tp'), may hold values from -0.125 to 0.125
- query_proj: bfloat16 [2048, 1024], P(None, 'tp'), may hold values from -0.21875 to 0.21875
- key_proj: bfloat16 [2048, 1024], P(None, 'tp'), may hold values from -0.21875 to 0.21875
- value_proj: bfloat16 [2048, 1024], P(None, 'tp'), may hold values from -0.125 to 0.125
- filter_taps: bfloat16 [3, 1024], P(None, 'tp'), may hold values from -3.5 to 3.5
- break_bias: bfloat16 [16384, 16], P('sp', 'tp'), may hold values from -18 to 0
- filter_readout: bfloat16 [1024, 2048], replicated, may hold values from -0.125 to 0.125
- attention_readout: bfloat16 [1024, 2048], replicated, may hold values from -0.125 to 0.125
Outputs:
- mixed: bfloat16 [16384, 2048], P(('sp', 'tp'))
- mass_logarithm: float32 [16, 16384], P('tp', 'sp')
The draws below stay inside these ranges and needn't reach their ends.
All inputs are finite; a program needn't handle non-finite values.
Results may differ from the reference program's by a relative error of at most 0.013.
Values may be sent and summed in bfloat16 or wider, within the bound.
A program may use at most 128 MiB of HBM per device.

```python
import math
import jax
import jax.numpy as jnp
from jax import lax

D = 2048
CONV_WIDTH = 1024
HEAD_COUNT = 16
HEAD_DIM = 64
CONV_W = 3
TOK_DEV = 1024
ATT_WIDTH = 1024
TOKEN_COUNT = 16384
N_SP = 16


def draw_tokens(key, part):
    row_scale = jnp.exp(jax.random.uniform(jax.random.fold_in(key, 11), (TOKEN_COUNT, 1), jnp.float32, math.log(0.3), math.log(3.0)))
    col_scale = jnp.exp(jnp.linspace(math.log(0.4), math.log(2.5), D) + jax.random.uniform(jax.random.fold_in(key, 12), (D,), jnp.float32, -0.4, 0.4))
    base = jax.random.normal(jax.random.fold_in(key, 13), (TOKEN_COUNT, D), jnp.float32)
    value_matrix = jnp.clip(base * row_scale * col_scale[None, :], -16.0, 16.0)
    return value_matrix.astype(jnp.bfloat16)


def draw_break_bias(key, part):
    head_rank = jax.random.permutation(jax.random.fold_in(key, 21), HEAD_COUNT)
    slow_heads = head_rank < HEAD_COUNT // 2
    slow_rate = jax.random.uniform(jax.random.fold_in(key, 22), (HEAD_COUNT,), jnp.float32, 0.25, 1.0) / TOKEN_COUNT
    span_low = max(2.0, min(30.0, TOK_DEV / 8.0))
    span_high = max(4.0, min(100.0, TOK_DEV / 3.0))
    fast_span = jax.random.uniform(jax.random.fold_in(key, 23), (HEAD_COUNT,), jnp.float32, span_low, span_high)
    break_rate = jnp.where(slow_heads, slow_rate, 1.0 / fast_span)
    block_count = TOKEN_COUNT // TOK_DEV
    block_factor = jax.random.uniform(jax.random.fold_in(key, 24), (block_count, HEAD_COUNT), jnp.float32, -0.7, 0.7)
    blockwise = jnp.repeat(block_factor, TOK_DEV, axis=0)
    rough = jax.random.uniform(jax.random.fold_in(key, 25), (TOKEN_COUNT, HEAD_COUNT), jnp.float32, -0.5, 0.5)
    value_matrix = jnp.log(break_rate)[None, :] - 4.5 + blockwise + rough
    spike_places = jax.random.randint(jax.random.fold_in(key, 26), (4,), 0, TOKEN_COUNT)
    spike_found = jnp.any(jnp.arange(TOKEN_COUNT)[:, None] == spike_places[None, :], axis=1)
    spike_value = jax.random.uniform(jax.random.fold_in(key, 27), (TOKEN_COUNT, HEAD_COUNT), jnp.float32, -1.5, 0.0)
    value_matrix = jnp.where(spike_found[:, None], spike_value, value_matrix)
    value_matrix = jnp.clip(value_matrix, -18.0, 0.0)
    return value_matrix.astype(jnp.bfloat16)


def shard_levels(key, shape, pieces, low, largest):
    level, own = 1.0, jax.random.fold_in(key, 6)
    for dim, shards_of in pieces:
        heights = jnp.exp(jax.random.uniform(jax.random.fold_in(own, dim), (shards_of,), jnp.float32, low / len(pieces), largest / len(pieces)))
        level = level * jnp.repeat(heights, shape[dim] // shards_of).reshape([-1 if axis == dim else 1 for axis in range(len(shape))])
    return level


def gaussian(own_key, extent, width, limit, shards=(), kind=jnp.bfloat16):
    factor_of = shard_levels(own_key, extent, shards, -0.22, 0.18) if shards else 1.0
    values = jax.random.normal(own_key, extent, jnp.float32) * width * factor_of
    return jnp.minimum(jnp.maximum(values, -limit), limit).astype(kind)


def setup_inputs(seed: int = 0) -> dict:
    key_list = jax.random.split(jax.random.key(seed), 13)
    return {
        "tokens": draw_tokens(jax.random.fold_in(key_list[12], 71), 0),
        "norm_gain": jnp.clip(1.0 + 0.18 * jax.random.normal(key_list[1], (D,), jnp.float32), 0.1, 1.9),
        "signal_proj": gaussian(key_list[2], (D, CONV_WIDTH), D ** -0.5, 0.125, ((1, 8),)),
        "postgate_proj": gaussian(key_list[3], (D, CONV_WIDTH), D ** -0.5, 0.125, ((1, 8),)),
        "pregate_proj": gaussian(key_list[4], (D, CONV_WIDTH), D ** -0.5, 0.125, ((1, 8),)),
        "query_proj": gaussian(key_list[5], (D, ATT_WIDTH), (D // 3) ** -0.5, 0.21875, ((1, 8),)),
        "key_proj": gaussian(key_list[6], (D, ATT_WIDTH), (D // 3) ** -0.5, 0.21875, ((1, 8),)),
        "value_proj": gaussian(key_list[7], (D, ATT_WIDTH), D ** -0.5, 0.125, ((1, 8),)),
        "filter_taps": gaussian(key_list[8], (CONV_W, CONV_WIDTH), CONV_W ** -0.5, 3.5, ((1, 8),)),
        "break_bias": draw_break_bias(jax.random.fold_in(key_list[12], 71), 0),
        "filter_readout": gaussian(key_list[10], (CONV_WIDTH, D), (CONV_WIDTH + ATT_WIDTH) ** -0.5, 0.125),
        "attention_readout": gaussian(key_list[11], (ATT_WIDTH, D), (CONV_WIDTH + ATT_WIDTH) ** -0.5, 0.125),
    }


epsilon = 1e-06
mass_floor = 0.1

def project(scaled, weight, inverse):
    product = jnp.dot(scaled, weight, preferred_element_type=jnp.float32)
    return (product * inverse[:, None]).astype(jnp.bfloat16)

def filter_mix(signal, post_gate, pre_gate, filter_taps):
    product = pre_gate.astype(jnp.float32) * signal.astype(jnp.float32)
    padded = jnp.concatenate([jnp.zeros((CONV_W - 1, product.shape[1]), jnp.float32), product], axis=0)
    length = product.shape[0]
    tap_values = filter_taps.astype(jnp.float32)
    running = jnp.zeros_like(product)
    for offset in range(CONV_W):
        running = running + tap_values[offset][None, :] * padded[offset:offset + length]
    return (post_gate.astype(jnp.float32) * running).astype(jnp.bfloat16)

def head_attention(operands):
    queries, key_rows, value_rows, bias_row = operands
    outputs = []
    remains = []
    score_scale = HEAD_DIM ** (-0.5)
    for segment in range(N_SP):
        prefix_blocks = segment + 1
        query_block = queries[segment * TOK_DEV:(segment + 1) * TOK_DEV].astype(jnp.float32)
        key_blocks = key_rows[:prefix_blocks * TOK_DEV].astype(jnp.float32).reshape(prefix_blocks, TOK_DEV, HEAD_DIM)
        value_blocks = value_rows[:prefix_blocks * TOK_DEV].astype(jnp.float32).reshape(prefix_blocks, TOK_DEV, HEAD_DIM)
        bias_blocks = bias_row[:prefix_blocks * TOK_DEV].reshape(prefix_blocks, TOK_DEV)
        scores = jnp.einsum('td,nsd->nts', query_block, key_blocks) * score_scale + bias_blocks[:, None, :]
        block_ids = jnp.arange(prefix_blocks)[:, None, None]
        row_ids = jnp.arange(TOK_DEV)[None, :, None]
        col_ids = jnp.arange(TOK_DEV)[None, None, :]
        allowed = (block_ids < segment) | (col_ids < row_ids)
        log_remainder = jnp.where(allowed, jax.nn.log_sigmoid(-scores), 0.0)
        running = jnp.cumsum(log_remainder, axis=2)
        block_total = running[:, :, -1:]
        later_sum = block_total - running
        weights = jnp.where(allowed, jnp.exp(jax.nn.log_sigmoid(scores) + later_sum), 0.0).astype(jnp.bfloat16)
        partial_value = jnp.einsum('nts,nsd->ntd', weights.astype(jnp.float32), value_blocks)
        totals = block_total[:, :, 0]
        carried = lax.optimization_barrier(jnp.sum(totals, axis=0))[None, :] - jnp.cumsum(totals, axis=0)
        outputs.append(lax.optimization_barrier(jnp.sum(partial_value * jnp.exp(carried)[:, :, None], axis=0)))
        remains.append(lax.optimization_barrier(jnp.sum(totals, axis=0)))
    return (jnp.concatenate(outputs, axis=0), jnp.concatenate(remains, axis=0))

def reference(tokens, norm_gain, signal_proj, postgate_proj, pregate_proj, query_proj, key_proj, value_proj, filter_taps, break_bias, filter_readout, attention_readout):
    widened = tokens.astype(jnp.float32)
    inverse = lax.rsqrt(lax.optimization_barrier(jnp.mean(widened * widened, axis=1)) + epsilon)
    scaled = (widened * norm_gain.astype(jnp.float32)[None, :]).astype(jnp.bfloat16)
    signal = project(scaled, signal_proj, inverse)
    post_gate = project(scaled, postgate_proj, inverse)
    pre_gate = project(scaled, pregate_proj, inverse)
    queries = project(scaled, query_proj, inverse)
    key_rows = project(scaled, key_proj, inverse)
    value_rows = project(scaled, value_proj, inverse)
    filtered = filter_mix(signal, post_gate, pre_gate, filter_taps)
    query_heads = queries.reshape(TOKEN_COUNT, HEAD_COUNT, HEAD_DIM).transpose(1, 0, 2)
    key_heads = key_rows.reshape(TOKEN_COUNT, HEAD_COUNT, HEAD_DIM).transpose(1, 0, 2)
    value_heads = value_rows.reshape(TOKEN_COUNT, HEAD_COUNT, HEAD_DIM).transpose(1, 0, 2)
    bias_heads = break_bias.astype(jnp.float32).T
    head_out, head_remain = lax.map(head_attention, (query_heads, key_heads, value_heads, bias_heads))
    attended = head_out.transpose(1, 0, 2).reshape(TOKEN_COUNT, HEAD_COUNT * HEAD_DIM).astype(jnp.bfloat16)
    mass_logarithm = jnp.log(jnp.maximum(-jnp.expm1(head_remain), mass_floor))
    mixed = (jnp.dot(filtered, filter_readout, preferred_element_type=jnp.float32) + jnp.dot(attended, attention_readout, preferred_element_type=jnp.float32)).astype(jnp.bfloat16)
    return (mixed, mass_logarithm)
```

```python
import jax
import jax.numpy as jnp
from jax import lax
from jax.experimental import pallas as pl
from jax.experimental.pallas import tpu as pltpu
from jax.sharding import PartitionSpec as P

HEAD_DIM = 64
CONV_W = 3
CH = 256
NT = 4
CAP = 24.0
LOG2E = 1.4426950408889634
epsilon = 1e-06
mass_floor = 0.1


def scan_chunk(y_ref, carry_ref, w_ref, masked):
    groups = CH // 8
    seg = CH // 8
    if masked:
        row = lax.broadcasted_iota(jnp.int32, (8, CH), 0) * seg
        col = lax.broadcasted_iota(jnp.int32, (8, CH), 1)
        diff = col - row
    r = jnp.ones((8, CH), jnp.float32)
    for g in reversed(range(groups // 4)):
        us, ds = [], []
        for k in range(4):
            j = 4 * g + k
            y = y_ref[j * 8:(j + 1) * 8, :]
            u = jnp.exp2(jnp.minimum(y, CAP))
            if masked:
                u = jnp.where(diff > j, u, 0.0)
            us.append(u)
            ds.append(1.0 + u)
        prod = (ds[0] * ds[1]) * (ds[2] * ds[3])
        r = r * (1.0 / prod)
        e = r
        for k in range(4):
            j = 4 * g + k
            y_ref[j * 8:(j + 1) * 8, :] = us[k] * e
            if k < 3:
                e = e * ds[k]
    sub = lax.broadcasted_iota(jnp.int32, (8, CH), 0)
    s = r
    for k in (1, 2, 4):
        s = s * jnp.where(sub < 8 - k, pltpu.roll(s, 8 - k, 0), 1.0)
    excl = jnp.where(sub < 7, pltpu.roll(s, 7, 0), 1.0)
    carry = carry_ref[...]
    c = excl * carry
    carry_ref[...] = carry * jnp.broadcast_to(s[0:1, :], (8, CH))
    w = y_ref[...].reshape(CH // 8, 8, CH) * c[None]
    w_ref[...] = w.reshape(CH, CH).astype(jnp.bfloat16)

def qk(k_ref, q_ref, tile):
    kk = k_ref
    return jnp.dot(jnp.concatenate([kk, kk], axis=1), q_ref[:, tile * CH:(tile + 1) * CH],
                   preferred_element_type=jnp.float32)

def attend_set(qt, blk, kchunk, vchunk, acc, carry, ya, yb, wa, wb):
    base = 4 * blk
    for t in range(NT):
        acc[t] = jnp.zeros_like(acc[t])
        carry[t] = jnp.ones((8, CH), jnp.float32)
    for c in reversed(range(NT)):
        kk = kchunk(base + c)
        for t in range(c, NT):
            ya[t] = qk(kk, qt, t)
        for t in range(c, NT):
            scan_chunk(ya.at[t], carry.at[t], wb.at[t], t == c)
        if c > 0:
            vv = vchunk(base + c)
            for t in range(c, NT):
                acc[t] += jnp.dot(vv, wb[t], preferred_element_type=jnp.float32)
    kk = kchunk(jnp.maximum(base - 1, 0))
    for t in range(NT):
        ya[t] = qk(kk, qt, t)

    def half(c, ysrc, ydst, wdst, wsrc):
        kn = kchunk(jnp.maximum(c - 1, 0))
        vp = vchunk(c + 1)
        for t in range(NT):
            scan_chunk(ysrc.at[t], carry.at[t], wdst.at[t], False)
            ydst[t] = qk(kn, qt, t)
            acc[t] += jnp.dot(vp, wsrc[t], preferred_element_type=jnp.float32)

    def body(p, _):
        c = base - 1 - 2 * p
        half(c, ya, yb, wa, wb)
        half(c - 1, yb, ya, wb, wa)
        return 0
    lax.fori_loop(0, 2 * blk, body, 0)
    vp = vchunk(0)
    for t in range(NT):
        acc[t] += jnp.dot(vp, wb[t], preferred_element_type=jnp.float32)


def attention_kernel(qt, kp, vt, out, rem, acc, carry, ya, yb, wa, wb):
    me = lax.axis_index("sp")
    head = me // 8

    def kchunk(c):
        return kp[c // NT, head, pl.ds(pl.multiple_of((c % NT) * CH, CH), CH), :]

    def vchunk(c):
        return vt[c // NT, head, c % NT]

    for which in range(2):
        block = me if which == 0 else 15 - me
        attend_set(qt.at[which], block, kchunk, vchunk, acc, carry, ya, yb, wa, wb)
        for t in range(NT):
            out[which, :, t * CH:(t + 1) * CH] = acc[t].astype(jnp.bfloat16)
            rem[which, :, t * CH:(t + 1) * CH] = carry[t]


def attention(qt, kp, vt):
    vmem = pl.BlockSpec(memory_space=pltpu.VMEM)
    return pl.pallas_call(
        attention_kernel,
        out_shape=(jax.ShapeDtypeStruct((2, HEAD_DIM, NT * CH), jnp.bfloat16),
                   jax.ShapeDtypeStruct((2, 8, NT * CH), jnp.float32)),
        in_specs=[vmem] * 3,
        out_specs=(vmem, vmem),
        scratch_shapes=[
            pltpu.VMEM((NT, HEAD_DIM, CH), jnp.float32),
            pltpu.VMEM((NT, 8, CH), jnp.float32),
            pltpu.VMEM((NT, CH, CH), jnp.float32),
            pltpu.VMEM((NT, CH, CH), jnp.float32),
            pltpu.VMEM((NT, CH, CH), jnp.bfloat16),
            pltpu.VMEM((NT, CH, CH), jnp.bfloat16),
        ],
        compiler_params=pltpu.CompilerParams(vmem_limit_bytes=50 * 2**20),
    )(qt, kp, vt)


def strided(rows):
    n = rows.shape[0]
    return rows.reshape(n // CH, 8, CH // 8, -1).transpose(0, 2, 1, 3).reshape(n, -1)


def split_two(x):
    hi = x.astype(jnp.bfloat16)
    return hi, (x - hi.astype(jnp.float32)).astype(jnp.bfloat16)


def per_device(tokens, norm_gain, signal_proj, postgate_proj, pregate_proj, query_proj, key_proj,
               value_proj, filter_taps, break_bias, filter_readout, attention_readout):
    n = tokens.shape[0]
    me = lax.axis_index("sp")
    projections = (signal_proj, postgate_proj, pregate_proj, query_proj, key_proj, value_proj)
    whole_rows = lax.all_gather(tokens, "tp", axis=1, tiled=True)
    widened = whole_rows.astype(jnp.float32)
    inverse = lax.rsqrt(jnp.mean(widened * widened, axis=1) + epsilon)
    scaled = (widened * norm_gain[None, :]).astype(jnp.bfloat16)
    products = [jnp.dot(scaled, w, preferred_element_type=jnp.float32) for w in projections]
    signal, post_gate, pre_gate, queries, keys, values = [
        (p * inverse[:, None]).astype(jnp.bfloat16) for p in products]

    rim = CONV_W - 1
    product = pre_gate.astype(jnp.float32) * signal.astype(jnp.float32)
    before = lax.ppermute(product[n - rim:], "sp", [(i, i + 1) for i in range(15)])
    extended = jnp.concatenate([before, product], axis=0)
    taps = filter_taps.astype(jnp.float32)
    running = sum(taps[w][None, :] * extended[w:w + n] for w in range(CONV_W))
    filtered = (post_gate.astype(jnp.float32) * running).astype(jnp.bfloat16)

    mirror = [(i, 15 - i) for i in range(16)]
    mine = me // 8
    qrows = queries.T.reshape(2, HEAD_DIM, n)
    own_q = lax.dynamic_index_in_dim(qrows, mine, 0, False)
    other_q = lax.ppermute(lax.dynamic_index_in_dim(qrows, 1 - mine, 0, False), "sp", mirror)
    hi, lo = split_two(jnp.stack([own_q, other_q]).astype(jnp.float32) * (HEAD_DIM ** -0.5 * LOG2E))
    ones = jnp.ones((2, 2, n), jnp.bfloat16)
    qt = jnp.concatenate([hi, ones, jnp.zeros((2, 62, n), jnp.bfloat16), lo,
                          jnp.zeros((2, 64, n), jnp.bfloat16)], axis=1)
    bias_hi, bias_lo = split_two(break_bias.astype(jnp.float32) * LOG2E)
    pad = jnp.zeros((n, 62), jnp.bfloat16)
    kp = jnp.stack([strided(jnp.concatenate(
        [keys[:, h * 64:(h + 1) * 64], bias_hi[:, h:h + 1], bias_lo[:, h:h + 1], pad], axis=1))
        for h in range(2)])
    vt = strided(values).reshape(NT, CH, 2, HEAD_DIM).transpose(2, 0, 3, 1)
    all_kp = lax.all_gather(kp, "sp")
    all_vt = lax.all_gather(vt, "sp")
    out, rem = attention(qt, all_kp, all_vt)
    back_out = lax.ppermute(out[1], "sp", mirror)
    back_rem = lax.ppermute(rem[1, :1], "sp", mirror)

    def arranged(own, back):
        return jnp.where(mine == 0, jnp.concatenate([own, back], 0), jnp.concatenate([back, own], 0))

    attended = arranged(out[0], back_out).T
    mass_logarithm = jnp.log(jnp.maximum(1.0 - arranged(rem[0, :1], back_rem), mass_floor))
    filter_rows = lax.all_to_all(filtered, "tp", split_axis=0, concat_axis=1, tiled=True)
    attended_rows = lax.all_to_all(attended, "tp", split_axis=0, concat_axis=1, tiled=True)
    mixed = (jnp.dot(filter_rows, filter_readout, preferred_element_type=jnp.float32)
             + jnp.dot(attended_rows, attention_readout, preferred_element_type=jnp.float32)).astype(jnp.bfloat16)
    return (mixed, mass_logarithm)


def solution(mesh):
    placed = (P("sp", "tp"), P()) + (P(None, "tp"),) * 7 + (P("sp", "tp"), P(), P())
    return jax.shard_map(per_device, mesh=mesh, in_specs=placed,
                         out_specs=(P(("sp", "tp"), None), P("tp", "sp")), check_vma=False)
```

```python
import jax
import jax.numpy as jnp
from jax import lax
from jax.experimental import pallas as pl
from jax.experimental.pallas import tpu as pltpu
from jax.sharding import PartitionSpec as P

HEAD_DIM = 64
CONV_W = 3
CH = 256
NT = 4
CAP = 24.0
LOG2E = 1.4426950408889634
epsilon = 1e-06
mass_floor = 0.1


def scan_chunk(y_ref, carry_ref, w_ref, masked):
    groups = CH // 8
    seg = CH // 8
    if masked:
        row = lax.broadcasted_iota(jnp.int32, (8, CH), 0) * seg
        col = lax.broadcasted_iota(jnp.int32, (8, CH), 1)
        diff = col - row
    r = jnp.ones((8, CH), jnp.float32)
    for g in reversed(range(groups // 4)):
        us, ds = [], []
        for k in range(4):
            j = 4 * g + k
            y = y_ref[j * 8:(j + 1) * 8, :]
            u = jnp.exp2(jnp.minimum(y, CAP))
            if masked:
                u = jnp.where(diff > j, u, 0.0)
            us.append(u)
            ds.append(1.0 + u)
        prod = (ds[0] * ds[1]) * (ds[2] * ds[3])
        r = r * (1.0 / prod)
        e = r
        for k in range(4):
            j = 4 * g + k
            y_ref[j * 8:(j + 1) * 8, :] = us[k] * e
            if k < 3:
                e = e * ds[k]
    sub = lax.broadcasted_iota(jnp.int32, (8, CH), 0)
    s = r
    for k in (1, 2, 4):
        s = s * jnp.where(sub < 8 - k, pltpu.roll(s, 8 - k, 0), 1.0)
    excl = jnp.where(sub < 7, pltpu.roll(s, 7, 0), 1.0)
    carry = carry_ref[...]
    c = excl * carry
    carry_ref[...] = carry * jnp.broadcast_to(s[0:1, :], (8, CH))
    w = y_ref[...].reshape(CH // 8, 8, CH) * c[None]
    w_ref[...] = w.reshape(CH, CH).astype(jnp.bfloat16)

def qk(k_ref, q_ref, tile):
    kk = k_ref
    return jnp.dot(jnp.concatenate([kk, kk], axis=1), q_ref[:, tile * CH:(tile + 1) * CH],
                   preferred_element_type=jnp.float32)

def attend_set(qt, blk, kchunk, vchunk, acc, carry, ya, yb, wa, wb):
    base = 4 * blk
    for t in range(NT):
        acc[t] = jnp.zeros_like(acc[t])
        carry[t] = jnp.ones((8, CH), jnp.float32)
    for c in reversed(range(NT)):
        kk = kchunk(base + c)
        for t in range(c, NT):
            ya[t] = qk(kk, qt, t)
        for t in range(c, NT):
            scan_chunk(ya.at[t], carry.at[t], wb.at[t], t == c)
        if c > 0:
            vv = vchunk(base + c)
            for t in range(c, NT):
                acc[t] += jnp.dot(vv, wb[t], preferred_element_type=jnp.float32)
    kk = kchunk(jnp.maximum(base - 1, 0))
    for t in range(NT):
        ya[t] = qk(kk, qt, t)

    def half(c, ysrc, ydst, wdst, wsrc):
        kn = kchunk(jnp.maximum(c - 1, 0))
        vp = vchunk(c + 1)
        for t in range(NT):
            scan_chunk(ysrc.at[t], carry.at[t], wdst.at[t], False)
            ydst[t] = qk(kn, qt, t)
            acc[t] += jnp.dot(vp, wsrc[t], preferred_element_type=jnp.float32)

    def body(p, _):
        c = base - 1 - 2 * p
        half(c, ya, yb, wa, wb)
        half(c - 1, yb, ya, wb, wa)
        return 0
    lax.fori_loop(0, 2 * blk, body, 0)
    vp = vchunk(0)
    for t in range(NT):
        acc[t] += jnp.dot(vp, wb[t], preferred_element_type=jnp.float32)


SP, TP = "sp", "tp"


def remote(src, dst, send, recv, sp, tp):
    return pltpu.make_async_remote_copy(src_ref=src, dst_ref=dst, send_sem=send, recv_sem=recv,
                                        device_id={SP: sp, TP: tp}, device_id_type=pl.DeviceIdType.MESH)


def query_place(z, x):
    flip = (z == 1) | (z == 3)
    column = jnp.where(flip, 3 - x, x)
    core = jnp.where((z == 1) | (z == 2), 1, 0)
    slot = jnp.where((z == 2) | (z == 3), 0, 1)
    return column, core, slot


def set_block(x, core, slot):
    return jnp.where(core == 0, jnp.where(slot == 0, 15 - x, x), jnp.where(slot == 0, 8 + x, 7 - x))


def attention_kernel(q, kp, vt, out, rem, kb, vb, qb, ob, rb, qt, acc, carry, ya, yb, wa, wb,
                     rk, rv, rq, ro, rr, sk, sv, sq, so, sr, xk, xv, dk, dv, fk):
    me = lax.axis_index(SP)
    t = lax.axis_index(TP)
    z, x = me // 4, me % 4
    core = t % 2
    partner = t + 1 - 2 * core
    active = core == z // 2
    right = z * 4 + (x + 1) % 4
    left = z * 4 + (x + 3) % 4

    col, qcore, slot = query_place(z, x)
    qtp = t - core + qcore

    def key_copy(l):
        g = 2 * core + l
        return (remote(kp.at[l], kb.at[me], sk.at[l], rk.at[me], g * 4 + x, t),
                remote(vt.at[l], vb.at[me], sv.at[l], rv.at[me], g * 4 + x, t))

    def query_copy(l):
        g = 2 * core + l
        return remote(q.at[l], qb.at[slot], sq.at[l], rq.at[slot], g * 4 + col, qtp)

    def query_local(l):
        g = 2 * core + l
        return (g == z) & (col == x) & (qcore == core)

    for l in range(2):
        @pl.when(2 * core + l != z)
        def _():
            for c in key_copy(l):
                c.start()

        @pl.when(jnp.logical_not(query_local(l)))
        def _():
            query_copy(l).start()

        @pl.when(2 * core + l == z)
        def _():
            kb[me] = kp[l]
            vb[me] = vt[l]

        @pl.when(query_local(l))
        def _():
            qb[slot] = q[l]

    def pass_on(b, to, ks, vs, keys=True, values=True, tp=t, src=None):
        ksrc, vsrc = src or (kb.at[b], vb.at[b])
        if keys:
            remote(ksrc, kb.at[b], ks, rk.at[b], to, tp).start()
        if values:
            remote(vsrc, vb.at[b], vs, rv.at[b], to, tp).start()

    def sent(b, to, ks, vs, keys=True, values=True, tp=t):
        if keys:
            remote(kb.at[b], kb.at[b], ks, rk.at[b], to, tp).wait_send()
        if values:
            remote(vb.at[b], vb.at[b], vs, rv.at[b], to, tp).wait_send()

    def arrived(b, keys=True, values=True):
        if keys:
            remote(kb.at[b], kb.at[b], sk.at[0], rk.at[b], me, t).wait_recv()
        if values:
            remote(vb.at[b], vb.at[b], sv.at[0], rv.at[b], me, t).wait_recv()

    @pl.when(active)
    def _():
        for zs in (3, 2, 1, 0):
            b = zs * 4 + x

            def spread(src):
                pass_on(b, right, xk.at[zs, 0], xv.at[zs, 0], src=src)
                pass_on(b, left, xk.at[zs, 1], xv.at[zs, 1], src=src)
                pass_on(b, me, dk.at[b], dv.at[b], tp=partner, src=src)

            @pl.when(z != zs)
            def _():
                arrived(b)
                spread(None)

            @pl.when(z == zs)
            def _():
                spread((kp.at[zs % 2], vt.at[zs % 2]))
        for zs in (3, 2, 1, 0):
            even = zs % 2 == 0
            b = zs * 4 + (x + 3) % 4
            arrived(b)
            pass_on(b, right, fk.at[zs, 0], fk.at[zs, 0], keys=even, values=not even)
            pass_on(b, me, dk.at[b], dv.at[b], tp=partner)
            b = zs * 4 + (x + 1) % 4
            arrived(b)
            pass_on(b, left, fk.at[zs, 1], fk.at[zs, 1], keys=not even, values=even)
            pass_on(b, me, dk.at[b], dv.at[b], tp=partner)
        for zs in (3, 2, 1, 0):
            b = zs * 4 + (x + 2) % 4
            arrived(b)
            pass_on(b, me, dk.at[b], dv.at[b], tp=partner)

    @pl.when(jnp.logical_not(active))
    def _():
        for b in range(16):
            arrived(b)

    def kchunk(c):
        return kb[c // NT, pl.ds(pl.multiple_of((c % NT) * CH, CH), CH), :]

    def vchunk(c):
        return vb[c // NT, c % NT]

    def result_copies(s):
        blk = set_block(x, core, s)
        back = t - core + z // 2
        return (remote(out_local.at[s], ob.at[z % 2], so.at[s], ro.at[z % 2], blk, back),
                remote(carry_out.at[s], rb.at[z % 2], sr.at[s], rr.at[z % 2], blk, back))

    out_local, carry_out = acc[1], acc[2]
    sums = acc[0]
    for s in range(2):
        blk = set_block(x, core, s)
        zb, xb = blk // 4, blk % 4
        own = (blk == me) & (core == z // 2)

        @pl.when(jnp.logical_not(own))
        def _():
            remote(qb.at[s], qb.at[s], sq.at[0], rq.at[s], me, t).wait_recv()
        qs = qb[s].astype(jnp.float32) * (HEAD_DIM ** -0.5 * LOG2E)
        hi = qs.astype(jnp.bfloat16)
        qt[0:64] = hi
        qt[64:128] = jnp.where(lax.broadcasted_iota(jnp.int32, (64, NT * CH), 0) < 2, 1.0, 0.0).astype(jnp.bfloat16)
        qt[128:192] = (qs - hi.astype(jnp.float32)).astype(jnp.bfloat16)
        qt[192:256] = jnp.zeros((64, NT * CH), jnp.bfloat16)
        attend_set(qt, blk, kchunk, vchunk, sums, carry, ya, yb, wa, wb)
        for i in range(NT):
            out_local[s, :, i * CH:(i + 1) * CH] = sums[i].astype(jnp.bfloat16)
            carry_out[s, :, i * CH:(i + 1) * CH] = carry[i]

        @pl.when(jnp.logical_not(own))
        def _():
            for c in result_copies(s):
                c.start()

        @pl.when(own)
        def _():
            ob[z % 2] = out_local[s]
            rb[z % 2] = carry_out[s]

    for l in range(2):
        @pl.when(jnp.logical_not(query_local(l)))
        def _():
            remote(ob.at[l], ob.at[l], so.at[0], ro.at[l], me, t).wait_recv()
            remote(rb.at[l], rb.at[l], sr.at[0], rr.at[l], me, t).wait_recv()
        out[l] = ob[l]
        rem[l] = rb[l]

    for l in range(2):
        @pl.when(2 * core + l != z)
        def _():
            for c in key_copy(l):
                c.wait_send()

        @pl.when(jnp.logical_not(query_local(l)))
        def _():
            query_copy(l).wait_send()

    @pl.when(active)
    def _():
        for zs in (3, 2, 1, 0):
            even = zs % 2 == 0
            b = zs * 4 + x
            sent(b, right, xk.at[zs, 0], xv.at[zs, 0])
            sent(b, left, xk.at[zs, 1], xv.at[zs, 1])
            sent(zs * 4 + (x + 3) % 4, right, fk.at[zs, 0], fk.at[zs, 0], keys=even, values=not even)
            sent(zs * 4 + (x + 1) % 4, left, fk.at[zs, 1], fk.at[zs, 1], keys=not even, values=even)
        for b in range(16):
            sent(b, me, dk.at[b], dv.at[b], tp=partner)

    for s in range(2):
        own = (set_block(x, core, s) == me) & (core == z // 2)

        @pl.when(jnp.logical_not(own))
        def _():
            for c in result_copies(s):
                c.wait_send()


def attention(q, kp, vt):
    vmem = pl.BlockSpec(memory_space=pltpu.VMEM)
    rows = NT * CH
    dma = pltpu.SemaphoreType.DMA
    return pl.pallas_call(
        attention_kernel,
        out_shape=(jax.ShapeDtypeStruct((2, HEAD_DIM, rows), jnp.bfloat16),
                   jax.ShapeDtypeStruct((2, 8, rows), jnp.float32)),
        in_specs=[vmem] * 3,
        out_specs=(vmem, vmem),
        scratch_shapes=[
            pltpu.VMEM((16, rows, 128), jnp.bfloat16),
            pltpu.VMEM((16, NT, HEAD_DIM, CH), jnp.bfloat16),
            pltpu.VMEM((2, HEAD_DIM, rows), jnp.bfloat16),
            pltpu.VMEM((2, HEAD_DIM, rows), jnp.bfloat16),
            pltpu.VMEM((2, 8, rows), jnp.float32),
            pltpu.VMEM((256, rows), jnp.bfloat16),
            (pltpu.VMEM((NT, HEAD_DIM, CH), jnp.float32), pltpu.VMEM((2, HEAD_DIM, rows), jnp.bfloat16),
             pltpu.VMEM((2, 8, rows), jnp.float32)),
            pltpu.VMEM((NT, 8, CH), jnp.float32),
            pltpu.VMEM((NT, CH, CH), jnp.float32),
            pltpu.VMEM((NT, CH, CH), jnp.float32),
            pltpu.VMEM((NT, CH, CH), jnp.bfloat16),
            pltpu.VMEM((NT, CH, CH), jnp.bfloat16),
            dma((16,)), dma((16,)), dma((2,)), dma((2,)), dma((2,)),
            dma((2,)), dma((2,)), dma((2,)), dma((2,)), dma((2,)),
            dma((4, 2)), dma((4, 2)), dma((16,)), dma((16,)), dma((4, 2)),
        ],
        compiler_params=pltpu.CompilerParams(vmem_limit_bytes=50 * 2**20, has_side_effects=True),
    )(q, kp, vt)


def strided(rows):
    n = rows.shape[0]
    return rows.reshape(n // CH, 8, CH // 8, -1).transpose(0, 2, 1, 3).reshape(n, -1)


def split_two(x):
    hi = x.astype(jnp.bfloat16)
    return hi, (x - hi.astype(jnp.float32)).astype(jnp.bfloat16)


def per_device(tokens, norm_gain, signal_proj, postgate_proj, pregate_proj, query_proj, key_proj,
               value_proj, filter_taps, break_bias, filter_readout, attention_readout):
    n = tokens.shape[0]
    projections = (signal_proj, postgate_proj, pregate_proj, query_proj, key_proj, value_proj)
    whole_rows = lax.all_gather(tokens, "tp", axis=1, tiled=True)
    widened = whole_rows.astype(jnp.float32)
    inverse = lax.rsqrt(jnp.mean(widened * widened, axis=1) + epsilon)
    scaled = (widened * norm_gain[None, :]).astype(jnp.bfloat16)
    products = [jnp.dot(scaled, w, preferred_element_type=jnp.float32) for w in projections]
    signal, post_gate, pre_gate, queries, keys, values = [
        (p * inverse[:, None]).astype(jnp.bfloat16) for p in products]

    rim = CONV_W - 1
    product = pre_gate.astype(jnp.float32) * signal.astype(jnp.float32)
    before = lax.ppermute(product[n - rim:], "sp", [(i, i + 1) for i in range(15)])
    extended = jnp.concatenate([before, product], axis=0)
    taps = filter_taps.astype(jnp.float32)
    running = sum(taps[w][None, :] * extended[w:w + n] for w in range(CONV_W))
    filtered = (post_gate.astype(jnp.float32) * running).astype(jnp.bfloat16)

    q = queries.T.reshape(2, HEAD_DIM, n)
    bias_hi, bias_lo = split_two(break_bias.astype(jnp.float32) * LOG2E)
    pad = jnp.zeros((n, 62), jnp.bfloat16)
    kp = jnp.stack([strided(jnp.concatenate(
        [keys[:, h * 64:(h + 1) * 64], bias_hi[:, h:h + 1], bias_lo[:, h:h + 1], pad], axis=1))
        for h in range(2)])
    vt = strided(values).reshape(NT, CH, 2, HEAD_DIM).transpose(2, 0, 3, 1)
    out, rem = attention(q, kp, vt)
    attended = out.reshape(2 * HEAD_DIM, n).T
    mass_logarithm = jnp.log(jnp.maximum(1.0 - rem[:, 0], mass_floor))
    filter_rows = lax.all_to_all(filtered, "tp", split_axis=0, concat_axis=1, tiled=True)
    attended_rows = lax.all_to_all(attended, "tp", split_axis=0, concat_axis=1, tiled=True)
    mixed = (jnp.dot(filter_rows, filter_readout, preferred_element_type=jnp.float32)
             + jnp.dot(attended_rows, attention_readout, preferred_element_type=jnp.float32)).astype(jnp.bfloat16)
    return (mixed, mass_logarithm)


def solution(mesh):
    placed = (P("sp", "tp"), P()) + (P(None, "tp"),) * 7 + (P("sp", "tp"), P(), P())
    return jax.shard_map(per_device, mesh=mesh, in_specs=placed,
                         out_specs=(P(("sp", "tp"), None), P("tp", "sp")), check_vma=False)
```

```python
import jax
import jax.numpy as jnp
from jax import lax
from jax.experimental import pallas as pl
from jax.experimental.pallas import tpu as pltpu
from jax.sharding import PartitionSpec as P

HEAD_DIM = 64
CONV_W = 3
CH = 256
NT = 4
CAP = 24.0
LOG2E = 1.4426950408889634
epsilon = 1e-06
mass_floor = 0.1


def scan_chunk(y_ref, carry_ref, w_ref, masked):
    groups = CH // 8
    seg = CH // 8
    if masked:
        row = lax.broadcasted_iota(jnp.int32, (8, CH), 0) * seg
        col = lax.broadcasted_iota(jnp.int32, (8, CH), 1)
        diff = col - row
    r = jnp.ones((8, CH), jnp.float32)
    for g in reversed(range(groups // 4)):
        us, ds = [], []
        for k in range(4):
            j = 4 * g + k
            y = y_ref[j * 8:(j + 1) * 8, :]
            u = jnp.exp2(jnp.minimum(y, CAP))
            if masked:
                u = jnp.where(diff > j, u, 0.0)
            us.append(u)
            ds.append(1.0 + u)
        prod = (ds[0] * ds[1]) * (ds[2] * ds[3])
        r = r * (1.0 / prod)
        e = r
        for k in range(4):
            j = 4 * g + k
            y_ref[j * 8:(j + 1) * 8, :] = us[k] * e
            if k < 3:
                e = e * ds[k]
    sub = lax.broadcasted_iota(jnp.int32, (8, CH), 0)
    s = r
    for k in (1, 2, 4):
        s = s * jnp.where(sub < 8 - k, pltpu.roll(s, 8 - k, 0), 1.0)
    excl = jnp.where(sub < 7, pltpu.roll(s, 7, 0), 1.0)
    carry = carry_ref[...]
    c = excl * carry
    carry_ref[...] = carry * jnp.broadcast_to(s[0:1, :], (8, CH))
    w = y_ref[...].reshape(CH // 8, 8, CH) * c[None]
    w_ref[...] = w.reshape(CH, CH).astype(jnp.bfloat16)

def qk(k_ref, q_ref, tile):
    kk = k_ref
    return jnp.dot(jnp.concatenate([kk, kk], axis=1), q_ref[:, tile * CH:(tile + 1) * CH],
                   preferred_element_type=jnp.float32)

def attend_set(qt, blk, kchunk, vchunk, acc, carry, ya, yb, wa, wb):
    base = 4 * blk
    for t in range(NT):
        acc[t] = jnp.zeros_like(acc[t])
        carry[t] = jnp.ones((8, CH), jnp.float32)
    for c in reversed(range(NT)):
        kk = kchunk(base + c)
        for t in range(c, NT):
            ya[t] = qk(kk, qt, t)
        for t in range(c, NT):
            scan_chunk(ya.at[t], carry.at[t], wb.at[t], t == c)
        if c > 0:
            vv = vchunk(base + c)
            for t in range(c, NT):
                acc[t] += jnp.dot(vv, wb[t], preferred_element_type=jnp.float32)
    kk = kchunk(jnp.maximum(base - 1, 0))
    for t in range(NT):
        ya[t] = qk(kk, qt, t)

    def half(c, ysrc, ydst, wdst, wsrc):
        kn = kchunk(jnp.maximum(c - 1, 0))
        vp = vchunk(c + 1)
        for t in range(NT):
            scan_chunk(ysrc.at[t], carry.at[t], wdst.at[t], False)
            ydst[t] = qk(kn, qt, t)
            acc[t] += jnp.dot(vp, wsrc[t], preferred_element_type=jnp.float32)

    def body(p, _):
        c = base - 1 - 2 * p
        half(c, ya, yb, wa, wb)
        half(c - 1, yb, ya, wb, wa)
        return 0
    lax.fori_loop(0, 2 * blk, body, 0)
    vp = vchunk(0)
    for t in range(NT):
        acc[t] += jnp.dot(vp, wb[t], preferred_element_type=jnp.float32)


SP, TP = "sp", "tp"
ROWS = NT * CH


def remote(src, dst, send, recv, sp, tp):
    return pltpu.make_async_remote_copy(src_ref=src, dst_ref=dst, send_sem=send, recv_sem=recv,
                                        device_id={SP: sp, TP: tp}, device_id_type=pl.DeviceIdType.MESH)


def query_place(z, x):
    column = jnp.where((z == 1) | (z == 3), 3 - x, x)
    core = jnp.where((z == 1) | (z == 2), 1, 0)
    slot = jnp.where((z == 2) | (z == 3), 0, 1)
    return column, core, slot


def set_block(x, core, slot):
    return jnp.where(core == 0, jnp.where(slot == 0, 15 - x, x), jnp.where(slot == 0, 8 + x, 7 - x))


def layer_kernel(tokens, gain, w0, w1, w2, w3, w4, w5, taps, bias, fr_hbm, ar_hbm, mixed, mass,
                 tk, wts, fr, ar, sc, pr, post, fl, q, kp, vt, kb, vb, qb, rb, fa, at, total,
                 qt, out_local, carry_out, sums, carry, ya, yb, wa, wb,
                 lw, st, rt, sf, rim,
                 rk, rv, rq, ro, rr, sk, sv, sq, so, sr, xk, xv, dk, dv, fk, sx, rx):
    me = lax.axis_index(SP)
    t = lax.axis_index(TP)
    z, x = me // 4, me % 4
    core = t % 2
    y = t // 2
    partner = t + 1 - 2 * core
    active = core == z // 2
    right = z * 4 + (x + 1) % 4
    left = z * 4 + (x + 3) % 4

    local = [pltpu.make_async_copy(w, wts.at[:, i * 128:(i + 1) * 128], lw.at[i])
             for i, w in enumerate((w0, w1, w2, w3, w4, w5))]
    local += [pltpu.make_async_copy(fr_hbm, fr, lw.at[6]), pltpu.make_async_copy(ar_hbm, ar, lw.at[7])]

    up = (t + 2) % 8
    down = (t + 6) % 8
    far = (t + 4) % 8

    def rows(k):
        return pl.ds(k * CH, CH)

    def feature_sends(k):
        src = tokens.at[rows(k)]
        dst = tk.at[t, rows(k)]
        return [remote(src, dst, st.at[k, 0], rt.at[t, k], me, up),
                remote(src, dst, st.at[k, 1], rt.at[t, k], me, down),
                remote(src, dst, st.at[k, 2], rt.at[t, k], me, partner)]

    def relay(k):
        slot, to = (down, up) if k % 2 == 0 else (up, down)
        part = tk.at[slot, rows(k)]
        return remote(part, part, st.at[k, 3], rt.at[slot, k], me, to)

    def over(k, n, slot):
        part = tk.at[slot, rows(k)]
        return remote(part, part, st.at[k, 4 + n], rt.at[slot, k], me, partner)

    def got(slot, k):
        part = tk.at[slot, rows(k)]
        remote(part, part, st.at[k, 0], rt.at[slot, k], me, t).wait_recv()

    def near(k):
        got(down, k)
        got(up, k)
        relay(k).start()
        over(k, 0, down).start()
        over(k, 1, up).start()
        if k + 2 < NT:
            for c in feature_sends(k + 2):
                c.start()

    def rest(k):
        got(far, k)
        over(k, 2, far).start()
        for n in (0, 2, 4, 6):
            got((partner + n) % 8, k)

    rowi = lax.broadcasted_iota(jnp.int32, (CH, CH), 0)
    coli = lax.broadcasted_iota(jnp.int32, (CH, CH), 1)
    order = jnp.where(coli == (rowi % 8) * (CH // 8) + rowi // 8, 1.0, 0.0).astype(jnp.bfloat16)
    lane = lax.broadcasted_iota(jnp.int32, (CH, 128), 1)

    def project(k):
        r = rows(k)
        squares = jnp.zeros((CH, 128), jnp.float32)
        for s in range(8):
            v = tk[s, r, :].astype(jnp.float32)
            v2 = v * v
            squares = squares + v2[:, :128] + v2[:, 128:]
            sc[:, s * 256:(s + 1) * 256] = (v * gain[:, s * 256:(s + 1) * 256]).astype(jnp.bfloat16)
        inverse = lax.rsqrt(jnp.sum(squares, axis=1, keepdims=True) * (1.0 / 2048.0) + epsilon)

        def product(n):
            p = jnp.dot(sc[...], wts[:, n * 256:(n + 1) * 256], preferred_element_type=jnp.float32)
            p = (p * inverse).astype(jnp.bfloat16)
            return p[:, :128], p[:, 128:]

        signal, post_gate = product(0)
        pre_gate, queries = product(1)
        keys, values = product(2)
        pr[8 + k * CH:8 + (k + 1) * CH, :] = pre_gate.astype(jnp.float32) * signal.astype(jnp.float32)
        post[r, :] = post_gate
        q[:, r] = queries.astype(jnp.float32).T.astype(jnp.bfloat16)
        b = bias[r, :].astype(jnp.float32) * LOG2E
        wide = []
        for l in range(2):
            bl = b[:, l:l + 1]
            hi = bl.astype(jnp.bfloat16).astype(jnp.float32)
            kf = keys.astype(jnp.float32)
            if l == 1:
                kf = pltpu.roll(kf, 64, 1)
            extra = jnp.where(lane == 64, hi, jnp.where(lane == 65, bl - hi, 0.0))
            wide.append(jnp.where(lane < 64, kf, extra).astype(jnp.bfloat16))
        kk = jnp.dot(order, jnp.concatenate(wide, axis=1), preferred_element_type=jnp.float32).astype(jnp.bfloat16)
        kp[0, r, :] = kk[:, :128]
        kp[1, r, :] = kk[:, 128:]
        vv = jnp.dot(order, values, preferred_element_type=jnp.float32).T.astype(jnp.bfloat16)
        vt[0, k] = vv[:64]
        vt[1, k] = vv[64:]

    for k in range(2):
        for c in feature_sends(k):
            c.start()
    for c in local:
        c.start()
    tk[t] = tokens[...]
    near(0)
    near(1)
    rest(0)
    for c in local[:6]:
        c.wait()
    project(0)
    near(2)
    rest(1)
    project(1)
    near(3)
    rest(2)
    project(2)
    rest(3)
    project(3)

    col, qcore, slot = query_place(z, x)
    qtp = t - core + qcore

    def key_copy(l):
        g = 2 * core + l
        return (remote(kp.at[l], kb.at[me], sk.at[l], rk.at[me], g * 4 + x, t),
                remote(vt.at[l], vb.at[me], sv.at[l], rv.at[me], g * 4 + x, t))

    def query_copy(l):
        g = 2 * core + l
        return remote(q.at[pl.ds(l * 64, 64)], qb.at[slot], sq.at[l], rq.at[slot], g * 4 + col, qtp)

    def query_local(l):
        g = 2 * core + l
        return (g == z) & (col == x) & (qcore == core)

    for l in range(2):
        @pl.when(2 * core + l != z)
        def _():
            for c in key_copy(l):
                c.start()

        @pl.when(jnp.logical_not(query_local(l)))
        def _():
            query_copy(l).start()

        @pl.when(2 * core + l == z)
        def _():
            kb[me] = kp[l]
            vb[me] = vt[l]

        @pl.when(query_local(l))
        def _():
            qb[slot] = q[l * 64:(l + 1) * 64, :]

    def rim_copy():
        return remote(pr.at[pl.ds(ROWS, 8)], pr.at[pl.ds(0, 8)], rim.at[0], rim.at[1], (me + 1) % 16, t)

    @pl.when(me < 15)
    def _():
        rim_copy().start()

    def pass_on(b, to, ks, vs, keys=True, values=True, tp=t, src=None):
        ksrc, vsrc = src or (kb.at[b], vb.at[b])
        if keys:
            remote(ksrc, kb.at[b], ks, rk.at[b], to, tp).start()
        if values:
            remote(vsrc, vb.at[b], vs, rv.at[b], to, tp).start()

    def sent(b, to, ks, vs, keys=True, values=True, tp=t):
        if keys:
            remote(kb.at[b], kb.at[b], ks, rk.at[b], to, tp).wait_send()
        if values:
            remote(vb.at[b], vb.at[b], vs, rv.at[b], to, tp).wait_send()

    def arrived(b):
        remote(kb.at[b], kb.at[b], sk.at[0], rk.at[b], me, t).wait_recv()
        remote(vb.at[b], vb.at[b], sv.at[0], rv.at[b], me, t).wait_recv()

    @pl.when(active)
    def _():
        for zs in (3, 2, 1, 0):
            b = zs * 4 + x

            def spread(src):
                pass_on(b, right, xk.at[zs, 0], xv.at[zs, 0], src=src)
                pass_on(b, left, xk.at[zs, 1], xv.at[zs, 1], src=src)
                pass_on(b, me, dk.at[b], dv.at[b], tp=partner, src=src)

            @pl.when(z != zs)
            def _():
                arrived(b)
                spread(None)

            @pl.when(z == zs)
            def _():
                spread((kp.at[zs % 2], vt.at[zs % 2]))

    @pl.when(me == 0)
    def _():
        pr[0:8, :] = jnp.zeros((8, 128), jnp.float32)

    @pl.when(me > 0)
    def _():
        rim_copy().wait_recv()
    tp_values = taps[...].astype(jnp.float32)
    running = jnp.zeros((ROWS, 128), jnp.float32)
    for w in range(CONV_W):
        running = running + tp_values[w:w + 1, :] * pr[6 + w:6 + w + ROWS, :]
    fl[...] = (post[...].astype(jnp.float32) * running).astype(jnp.bfloat16)

    @pl.when(me < 15)
    def _():
        rim_copy().wait_send()

    def lanes(i):
        return pl.ds(pl.multiple_of(i * 128, 128), 128)

    def filter_copy(n):
        p = (t + n) % 8
        return remote(fl.at[lanes(p)], fa.at[:, lanes(t)], sf.at[n], sf.at[8 + n], me, p)

    for n in range(1, 8):
        filter_copy(n).start()
    fa[:, lanes(t)] = fl[lanes(t), :]

    @pl.when(active)
    def _():
        for zs in (3, 2, 1, 0):
            even = zs % 2 == 0
            b = zs * 4 + (x + 3) % 4
            arrived(b)
            pass_on(b, right, fk.at[zs, 0], fk.at[zs, 0], keys=even, values=not even)
            pass_on(b, me, dk.at[b], dv.at[b], tp=partner)
            b = zs * 4 + (x + 1) % 4
            arrived(b)
            pass_on(b, left, fk.at[zs, 1], fk.at[zs, 1], keys=not even, values=even)
            pass_on(b, me, dk.at[b], dv.at[b], tp=partner)
        for zs in (3, 2, 1, 0):
            b = zs * 4 + (x + 2) % 4
            arrived(b)
            pass_on(b, me, dk.at[b], dv.at[b], tp=partner)

    @pl.when(jnp.logical_not(active))
    def _():
        for b in range(16):
            arrived(b)

    def kchunk(c):
        return kb[c // NT, pl.ds(pl.multiple_of((c % NT) * CH, CH), CH), :]

    def vchunk(c):
        return vb[c // NT, c % NT]

    back = t - core + z // 2
    head_rows = pl.ds(pl.multiple_of((4 * y + z) * 64, 64), 64)

    def piece_copy(s, blk, p):
        return remote(out_local.at[s, :, pl.ds(p * 128, 128)], at.at[head_rows], so.at[s, p],
                      ro.at[4 * y + z], blk, p)

    def rem_copy(s, blk):
        return remote(carry_out.at[s], rb.at[z % 2], sr.at[s], rr.at[z % 2], blk, back)

    for s in range(2):
        blk = set_block(x, core, s)
        own = (blk == me) & (core == z // 2)

        @pl.when(jnp.logical_not(own))
        def _():
            remote(qb.at[s], qb.at[s], sq.at[0], rq.at[s], me, t).wait_recv()
        qs = qb[s].astype(jnp.float32) * (HEAD_DIM ** -0.5 * LOG2E)
        hi = qs.astype(jnp.bfloat16)
        qt[0:64] = hi
        qt[64:128] = jnp.where(lax.broadcasted_iota(jnp.int32, (64, ROWS), 0) < 2, 1.0, 0.0).astype(jnp.bfloat16)
        qt[128:192] = (qs - hi.astype(jnp.float32)).astype(jnp.bfloat16)
        qt[192:256] = jnp.zeros((64, ROWS), jnp.bfloat16)
        attend_set(qt, blk, kchunk, vchunk, sums, carry, ya, yb, wa, wb)
        for i in range(NT):
            out_local[s, :, i * CH:(i + 1) * CH] = sums[i].astype(jnp.bfloat16)
            carry_out[s, :, i * CH:(i + 1) * CH] = carry[i]
        for p in range(8):
            here = (blk == me) & (t == p)

            @pl.when(jnp.logical_not(here))
            def _():
                piece_copy(s, blk, p).start()

            @pl.when(here)
            def _():
                at[head_rows, :] = out_local[s, :, p * 128:(p + 1) * 128]

        @pl.when(jnp.logical_not(own))
        def _():
            rem_copy(s, blk).start()

        @pl.when(own)
        def _():
            rb[z % 2] = carry_out[s]

    for n in range(1, 8):
        remote(fl.at[lanes(0)], fa.at[:, lanes((t - n + 8) % 8)], sf.at[n], sf.at[8 + n], me, t).wait_recv()
    local[6].wait()
    local[7].wait()
    for n in range(8):
        c = slice(n * 256, (n + 1) * 256)
        total[:, c] = jnp.dot(fa[...], fr[:, c], preferred_element_type=jnp.float32)
    for h in range(16):
        hz = h % 4
        column, hcore, _ = query_place(z, x)
        mine = (hz == z) & (column == x) & (2 * (h // 4) + hcore == t)

        @pl.when(jnp.logical_not(mine))
        def _():
            part = at.at[pl.ds(h * 64, 64)]
            remote(part, part, so.at[0, 0], ro.at[h], me, t).wait_recv()
    rows_t = at[...].astype(jnp.float32).T.astype(jnp.bfloat16)
    for n in range(8):
        c = slice(n * 256, (n + 1) * 256)
        mixed[:, c] = (total[:, c] + jnp.dot(rows_t, ar[:, c], preferred_element_type=jnp.float32)).astype(jnp.bfloat16)
    for l in range(2):
        @pl.when(jnp.logical_not(query_local(l)))
        def _():
            remote(rb.at[l], rb.at[l], sr.at[0], rr.at[l], me, t).wait_recv()
        mass[l:l + 1, :] = jnp.log(jnp.maximum(1.0 - rb[l, 0:1, :], mass_floor))

    for k in range(NT):
        for c in feature_sends(k):
            c.wait_send()
        relay(k).wait_send()
        for n, sl in enumerate((down, up, far)):
            over(k, n, sl).wait_send()
    for n in range(1, 8):
        filter_copy(n).wait_send()
    for l in range(2):
        @pl.when(2 * core + l != z)
        def _():
            for c in key_copy(l):
                c.wait_send()

        @pl.when(jnp.logical_not(query_local(l)))
        def _():
            query_copy(l).wait_send()

    @pl.when(active)
    def _():
        for zs in (3, 2, 1, 0):
            even = zs % 2 == 0
            b = zs * 4 + x
            sent(b, right, xk.at[zs, 0], xv.at[zs, 0])
            sent(b, left, xk.at[zs, 1], xv.at[zs, 1])
            sent(zs * 4 + (x + 3) % 4, right, fk.at[zs, 0], fk.at[zs, 0], keys=even, values=not even)
            sent(zs * 4 + (x + 1) % 4, left, fk.at[zs, 1], fk.at[zs, 1], keys=not even, values=even)
        for b in range(16):
            sent(b, me, dk.at[b], dv.at[b], tp=partner)

    for s in range(2):
        blk = set_block(x, core, s)
        own = (blk == me) & (core == z // 2)
        for p in range(8):
            @pl.when(jnp.logical_not((blk == me) & (t == p)))
            def _():
                piece_copy(s, blk, p).wait_send()

        @pl.when(jnp.logical_not(own))
        def _():
            rem_copy(s, blk).wait_send()


def per_device(tokens, norm_gain, signal_proj, postgate_proj, pregate_proj, query_proj, key_proj,
               value_proj, filter_taps, break_bias, filter_readout, attention_readout):
    vmem = pl.BlockSpec(memory_space=pltpu.VMEM)
    hbm = pl.BlockSpec(memory_space=pl.ANY)
    dma = pltpu.SemaphoreType.DMA
    bf16, f32 = jnp.bfloat16, jnp.float32
    return pl.pallas_call(
        layer_kernel,
        out_shape=(jax.ShapeDtypeStruct((128, 2048), bf16), jax.ShapeDtypeStruct((2, ROWS), f32)),
        in_specs=[vmem, vmem] + [hbm] * 6 + [vmem, vmem, hbm, hbm],
        out_specs=(vmem, vmem),
        scratch_shapes=[
            pltpu.VMEM((8, ROWS, 256), bf16),
            pltpu.VMEM((2048, 768), bf16),
            pltpu.VMEM((1024, 2048), bf16),
            pltpu.VMEM((1024, 2048), bf16),
            pltpu.VMEM((CH, 2048), bf16),
            pltpu.VMEM((ROWS + 8, 128), f32),
            pltpu.VMEM((ROWS, 128), bf16),
            pltpu.VMEM((ROWS, 128), bf16),
            pltpu.VMEM((128, ROWS), bf16),
            pltpu.VMEM((2, ROWS, 128), bf16),
            pltpu.VMEM((2, NT, 64, CH), bf16),
            pltpu.VMEM((16, ROWS, 128), bf16),
            pltpu.VMEM((16, NT, 64, CH), bf16),
            pltpu.VMEM((2, 64, ROWS), bf16),
            pltpu.VMEM((2, 8, ROWS), f32),
            pltpu.VMEM((128, 1024), bf16),
            pltpu.VMEM((1024, 128), bf16),
            pltpu.VMEM((128, 2048), f32),
            pltpu.VMEM((256, ROWS), bf16),
            pltpu.VMEM((2, 64, ROWS), bf16),
            pltpu.VMEM((2, 8, ROWS), f32),
            pltpu.VMEM((NT, 64, CH), f32),
            pltpu.VMEM((NT, 8, CH), f32),
            pltpu.VMEM((NT, CH, CH), f32),
            pltpu.VMEM((NT, CH, CH), f32),
            pltpu.VMEM((NT, CH, CH), bf16),
            pltpu.VMEM((NT, CH, CH), bf16),
            dma((8,)), dma((4, 8)), dma((8, 4)), dma((16,)), dma((2,)),
            dma((16,)), dma((16,)), dma((2,)), dma((16,)), dma((2,)),
            dma((2,)), dma((2,)), dma((2,)), dma((2, 8)), dma((2,)),
            dma((4, 2)), dma((4, 2)), dma((16,)), dma((16,)), dma((4, 2)), dma((2,)), dma((2,)),
        ],
        compiler_params=pltpu.CompilerParams(vmem_limit_bytes=60 * 2**20, has_side_effects=True),
    )(tokens, norm_gain.reshape(1, -1), signal_proj, postgate_proj, pregate_proj, query_proj, key_proj,
      value_proj, filter_taps, break_bias, filter_readout, attention_readout)


def solution(mesh):
    placed = (P("sp", "tp"), P()) + (P(None, "tp"),) * 7 + (P("sp", "tp"), P(), P())
    return jax.shard_map(per_device, mesh=mesh, in_specs=placed,
                         out_specs=(P(("sp", "tp"), None), P("tp", "sp")), check_vma=False)
```

```python
import jax
import jax.numpy as jnp
from jax import lax
from jax.experimental import pallas as pl
from jax.experimental.pallas import tpu as pltpu
from jax.sharding import PartitionSpec as P

HEAD_DIM = 64
CONV_W = 3
CH = 256
NT = 4
CAP = 24.0
LOG2E = 1.4426950408889634
epsilon = 1e-06
mass_floor = 0.1


def scan_chunk(y_ref, carry_ref, w_ref, masked):
    groups = CH // 8
    seg = CH // 8
    if masked:
        row = lax.broadcasted_iota(jnp.int32, (8, CH), 0) * seg
        col = lax.broadcasted_iota(jnp.int32, (8, CH), 1)
        diff = col - row
    r = jnp.ones((8, CH), jnp.float32)
    for g in reversed(range(groups // 4)):
        us, ds = [], []
        for k in range(4):
            j = 4 * g + k
            y = y_ref[j * 8:(j + 1) * 8, :]
            u = jnp.exp2(jnp.minimum(y, CAP))
            if masked:
                u = jnp.where(diff > j, u, 0.0)
            us.append(u)
            ds.append(1.0 + u)
        prod = (ds[0] * ds[1]) * (ds[2] * ds[3])
        r = r * (1.0 / prod)
        e = r
        for k in range(4):
            j = 4 * g + k
            y_ref[j * 8:(j + 1) * 8, :] = us[k] * e
            if k < 3:
                e = e * ds[k]
    sub = lax.broadcasted_iota(jnp.int32, (8, CH), 0)
    s = r
    for k in (1, 2, 4):
        s = s * jnp.where(sub < 8 - k, pltpu.roll(s, 8 - k, 0), 1.0)
    excl = jnp.where(sub < 7, pltpu.roll(s, 7, 0), 1.0)
    carry = carry_ref[...]
    c = excl * carry
    carry_ref[...] = carry * jnp.broadcast_to(s[0:1, :], (8, CH))
    w = y_ref[...].reshape(CH // 8, 8, CH) * c[None]
    w_ref[...] = w.reshape(CH, CH).astype(jnp.bfloat16)

def qk(k_ref, q_ref, tile):
    kk = k_ref
    return jnp.dot(jnp.concatenate([kk, kk], axis=1), q_ref[:, tile * CH:(tile + 1) * CH],
                   preferred_element_type=jnp.float32)

def attend_set(qt, blk, kchunk, vchunk, acc, carry, ya, yb, wa, wb):
    base = 4 * blk
    for t in range(NT):
        acc[t] = jnp.zeros_like(acc[t])
        carry[t] = jnp.ones((8, CH), jnp.float32)
    for c in reversed(range(NT)):
        kk = kchunk(base + c)
        for t in range(c, NT):
            ya[t] = qk(kk, qt, t)
        for t in range(c, NT):
            scan_chunk(ya.at[t], carry.at[t], wb.at[t], t == c)
        if c > 0:
            vv = vchunk(base + c)
            for t in range(c, NT):
                acc[t] += jnp.dot(vv, wb[t], preferred_element_type=jnp.float32)
    kk = kchunk(jnp.maximum(base - 1, 0))
    for t in range(NT):
        ya[t] = qk(kk, qt, t)

    def half(c, ysrc, ydst, wdst, wsrc):
        kn = kchunk(jnp.maximum(c - 1, 0))
        vp = vchunk(c + 1)
        for t in range(NT):
            scan_chunk(ysrc.at[t], carry.at[t], wdst.at[t], False)
            ydst[t] = qk(kn, qt, t)
            acc[t] += jnp.dot(vp, wsrc[t], preferred_element_type=jnp.float32)

    def body(p, _):
        c = base - 1 - 2 * p
        half(c, ya, yb, wa, wb)
        half(c - 1, yb, ya, wb, wa)
        return 0
    lax.fori_loop(0, 2 * blk, body, 0)
    vp = vchunk(0)
    for t in range(NT):
        acc[t] += jnp.dot(vp, wb[t], preferred_element_type=jnp.float32)


SP, TP = "sp", "tp"
ROWS = NT * CH


def remote(src, dst, send, recv, sp, tp):
    return pltpu.make_async_remote_copy(src_ref=src, dst_ref=dst, send_sem=send, recv_sem=recv,
                                        device_id={SP: sp, TP: tp}, device_id_type=pl.DeviceIdType.MESH)


def query_place(z, x):
    column = jnp.where((z == 1) | (z == 3), 3 - x, x)
    core = jnp.where((z == 1) | (z == 2), 1, 0)
    slot = jnp.where((z == 2) | (z == 3), 0, 1)
    return column, core, slot


def set_block(x, core, slot):
    return jnp.where(core == 0, jnp.where(slot == 0, 15 - x, x), jnp.where(slot == 0, 8 + x, 7 - x))


def layer_kernel(tokens, gain, w0, w1, w2, w3, w4, w5, taps, bias, fr_hbm, ar_hbm, mixed, mass,
                 tk, wts, fr, ar, sc, pr, post, fl, q, kvp, kvb, qb, rb, fa, at, total,
                 qt, out_local, carry_out, sums, carry, ya, yb, wa, wb,
                 lw, st, rt, sf, rim,
                 rk, rq, ro, rr, sk, sq, so, sr, xk, dk, fk):
    me = lax.axis_index(SP)
    t = lax.axis_index(TP)
    z, x = me // 4, me % 4
    core = t % 2
    y = t // 2
    partner = t + 1 - 2 * core
    active = core == z // 2
    right = z * 4 + (x + 1) % 4
    left = z * 4 + (x + 3) % 4

    back = t - core + z // 2
    col, qcore, slot = query_place(z, x)
    qtp = t - core + qcore

    def query_local(l):
        return (2 * core + l == z) & (col == x) & (qcore == core)

    barrier = pltpu.get_barrier_semaphore()

    def greet(sp, tp):
        pl.semaphore_signal(barrier, inc=1, device_id={SP: sp, TP: tp}, device_id_type=pl.DeviceIdType.MESH)

    for n in range(1, 8):
        greet(me, (t + n) % 8)
    greet(right, t)
    greet(left, t)
    for n in range(1, 4):
        greet((me + 4 * n) % 16, t)
    expected = 12
    for s in range(2):
        blk = set_block(x, core, s)

        @pl.when(jnp.logical_not((blk == me) & (core == z // 2)))
        def _():
            greet(blk, back)
        expected = expected + jnp.where(query_local(s), 0, 1)

    @pl.when(me > 0)
    def _():
        greet(me - 1, t)
    expected = expected + jnp.where(me < 15, 1, 0)

    local = [pltpu.make_async_copy(w, wts.at[:, i * 128:(i + 1) * 128], lw.at[i])
             for i, w in enumerate((w0, w1, w2, w3, w4, w5))]
    local += [pltpu.make_async_copy(fr_hbm, fr, lw.at[6]), pltpu.make_async_copy(ar_hbm, ar, lw.at[7])]

    up = (t + 2) % 8
    down = (t + 6) % 8
    far = (t + 4) % 8

    def rows(k):
        return pl.ds(k * CH, CH)

    def feature_sends(k):
        src = tokens.at[rows(k)]
        dst = tk.at[t, rows(k)]
        return [remote(src, dst, st.at[k, 0], rt.at[t, k], me, up),
                remote(src, dst, st.at[k, 1], rt.at[t, k], me, down),
                remote(src, dst, st.at[k, 2], rt.at[t, k], me, partner)]

    def relay(k):
        slot, to = (down, up) if k % 2 == 0 else (up, down)
        part = tk.at[slot, rows(k)]
        return remote(part, part, st.at[k, 3], rt.at[slot, k], me, to)

    def over(k, n, slot):
        part = tk.at[slot, rows(k)]
        return remote(part, part, st.at[k, 4 + n], rt.at[slot, k], me, partner)

    def got(slot, k):
        part = tk.at[slot, rows(k)]
        remote(part, part, st.at[k, 0], rt.at[slot, k], me, t).wait_recv()

    def near(k):
        got(down, k)
        got(up, k)
        relay(k).start()
        over(k, 0, down).start()
        over(k, 1, up).start()
        if k + 2 < NT:
            for c in feature_sends(k + 2):
                c.start()

    def rest(k):
        got(far, k)
        over(k, 2, far).start()
        for n in (0, 2, 4, 6):
            got((partner + n) % 8, k)

    rowi = lax.broadcasted_iota(jnp.int32, (CH, CH), 0)
    coli = lax.broadcasted_iota(jnp.int32, (CH, CH), 1)
    order = jnp.where(coli == (rowi % 8) * (CH // 8) + rowi // 8, 1.0, 0.0).astype(jnp.bfloat16)
    lane = lax.broadcasted_iota(jnp.int32, (CH, 128), 1)

    def project(k):
        r = rows(k)
        squares = jnp.zeros((CH, 128), jnp.float32)
        for s in range(8):
            v = tk[s, r, :].astype(jnp.float32)
            v2 = v * v
            squares = squares + v2[:, :128] + v2[:, 128:]
            sc[:, s * 256:(s + 1) * 256] = (v * gain[:, s * 256:(s + 1) * 256]).astype(jnp.bfloat16)
        inverse = lax.rsqrt(jnp.sum(squares, axis=1, keepdims=True) * (1.0 / 2048.0) + epsilon)

        def product(n):
            p = jnp.dot(sc[...], wts[:, n * 256:(n + 1) * 256], preferred_element_type=jnp.float32)
            p = (p * inverse).astype(jnp.bfloat16)
            return p[:, :128], p[:, 128:]

        signal, post_gate = product(0)
        pre_gate, queries = product(1)
        keys, values = product(2)
        pr[8 + k * CH:8 + (k + 1) * CH, :] = pre_gate.astype(jnp.float32) * signal.astype(jnp.float32)
        post[r, :] = post_gate
        q[:, r] = queries.astype(jnp.float32).T.astype(jnp.bfloat16)
        b = jnp.concatenate([bias[:, r].astype(jnp.float32) * LOG2E, jnp.zeros((6, CH), jnp.float32)], axis=0).T
        wide = []
        for l in range(2):
            bl = b[:, l:l + 1]
            hi = bl.astype(jnp.bfloat16).astype(jnp.float32)
            kf = keys.astype(jnp.float32)
            if l == 1:
                kf = pltpu.roll(kf, 64, 1)
            extra = jnp.where(lane == 64, hi, jnp.where(lane == 65, bl - hi, 0.0))
            wide.append(jnp.where(lane < 64, kf, extra).astype(jnp.bfloat16))
        kk = jnp.dot(order, jnp.concatenate(wide, axis=1), preferred_element_type=jnp.float32).astype(jnp.bfloat16)
        vv = jnp.dot(order, values, preferred_element_type=jnp.float32).T.astype(jnp.bfloat16)
        for l in range(2):
            kvp[l, k, 0:256, :] = kk[:, l * 128:(l + 1) * 128]
            kvp[l, k, 256:320, :] = vv[l * 64:(l + 1) * 64, :128]
            kvp[l, k, 320:384, :] = vv[l * 64:(l + 1) * 64, 128:]

    for c in local:
        c.start()
    tk[t] = tokens[...]
    pl.semaphore_wait(barrier, expected)
    for k in range(2):
        for c in feature_sends(k):
            c.start()

    def key_copy(l, k):
        g = 2 * core + l
        return remote(kvp.at[l, k], kvb.at[me, k], sk.at[l, k], rk.at[me, k], g * 4 + x, t)

    def send_keys(k):
        for l in range(2):
            @pl.when(2 * core + l != z)
            def _():
                key_copy(l, k).start()

            @pl.when(2 * core + l == z)
            def _():
                kvb[me, k] = kvp[l, k]

    def pass_on(b, k, to, sem, tp=t, src=None):
        return remote(kvb.at[b, k] if src is None else src, kvb.at[b, k], sem, rk.at[b, k], to, tp)

    def arrived(b, k):
        pass_on(b, k, me, sk.at[0, 0]).wait_recv()

    def own_column(k):
        @pl.when(active)
        def _():
            for zs in range(4):
                b = zs * 4 + x

                def spread(src):
                    pass_on(b, k, right, xk.at[zs, k, 0], src=src).start()
                    pass_on(b, k, left, xk.at[zs, k, 1], src=src).start()
                    pass_on(b, k, me, dk.at[b, k], partner, src=src).start()

                @pl.when(z != zs)
                def _():
                    arrived(b, k)
                    spread(None)

                @pl.when(z == zs)
                def _():
                    spread(kvp.at[zs % 2, k])

    def near_columns(k):
        @pl.when(active)
        def _():
            for zs in range(4):
                even = (zs + k) % 2 == 0
                b = zs * 4 + (x + 3) % 4
                arrived(b, k)
                if even:
                    pass_on(b, k, right, fk.at[zs, k]).start()
                pass_on(b, k, me, dk.at[b, k], partner).start()
                b = zs * 4 + (x + 1) % 4
                arrived(b, k)
                if not even:
                    pass_on(b, k, left, fk.at[zs, k]).start()
                pass_on(b, k, me, dk.at[b, k], partner).start()

    def far_column(k):
        @pl.when(active)
        def _():
            for zs in range(4):
                b = zs * 4 + (x + 2) % 4
                arrived(b, k)
                pass_on(b, k, me, dk.at[b, k], partner).start()

    near(0)
    near(1)
    rest(0)
    for c in local[:6]:
        c.wait()
    project(0)
    send_keys(0)
    near(2)
    rest(1)
    project(1)
    send_keys(1)
    own_column(0)
    near(3)
    rest(2)
    project(2)
    send_keys(2)
    own_column(1)
    near_columns(0)
    rest(3)
    project(3)
    send_keys(3)

    def query_copy(l):
        g = 2 * core + l
        return remote(q.at[pl.ds(l * 64, 64)], qb.at[slot], sq.at[l], rq.at[slot], g * 4 + col, qtp)

    for l in range(2):
        @pl.when(jnp.logical_not(query_local(l)))
        def _():
            query_copy(l).start()

        @pl.when(query_local(l))
        def _():
            qb[slot] = q[l * 64:(l + 1) * 64, :]

    def rim_copy():
        return remote(pr.at[pl.ds(ROWS, 8)], pr.at[pl.ds(0, 8)], rim.at[0], rim.at[1], (me + 1) % 16, t)

    @pl.when(me < 15)
    def _():
        rim_copy().start()

    own_column(2)
    near_columns(1)
    far_column(0)

    own_column(3)
    near_columns(2)
    far_column(1)

    @pl.when(me == 0)
    def _():
        pr[0:8, :] = jnp.zeros((8, 128), jnp.float32)

    @pl.when(me > 0)
    def _():
        rim_copy().wait_recv()
    tp_values = taps[...].astype(jnp.float32)
    running = jnp.zeros((ROWS, 128), jnp.float32)
    for w in range(CONV_W):
        running = running + tp_values[w:w + 1, :] * pr[6 + w:6 + w + ROWS, :]
    fl[...] = (post[...].astype(jnp.float32) * running).astype(jnp.bfloat16)

    @pl.when(me < 15)
    def _():
        rim_copy().wait_send()

    def lanes(i):
        return pl.ds(pl.multiple_of(i * 128, 128), 128)

    def filter_copy(n):
        p = (t + n) % 8
        return remote(fl.at[lanes(p)], fa.at[:, lanes(t)], sf.at[n], sf.at[8 + n], me, p)

    for n in range(1, 8):
        filter_copy(n).start()
    fa[:, lanes(t)] = fl[lanes(t), :]

    near_columns(3)
    far_column(2)
    far_column(3)

    @pl.when(jnp.logical_not(active))
    def _():
        for b in range(16):
            for k in range(NT):
                arrived(b, k)

    def kchunk(c):
        return kvb[c // NT, c % NT, 0:256, :]

    def vchunk(c):
        return jnp.concatenate([kvb[c // NT, c % NT, 256:320, :], kvb[c // NT, c % NT, 320:384, :]], axis=1)

    head_rows = pl.ds(pl.multiple_of((4 * y + z) * 64, 64), 64)

    def piece_copy(s, blk, p):
        return remote(out_local.at[s, :, pl.ds(p * 128, 128)], at.at[head_rows], so.at[s, p],
                      ro.at[4 * y + z], blk, p)

    def rem_copy(s, blk):
        return remote(carry_out.at[s], rb.at[z % 2], sr.at[s], rr.at[z % 2], blk, back)

    for s in range(2):
        blk = set_block(x, core, s)
        own = (blk == me) & (core == z // 2)

        @pl.when(jnp.logical_not(own))
        def _():
            remote(qb.at[s], qb.at[s], sq.at[0], rq.at[s], me, t).wait_recv()
        qs = qb[s].astype(jnp.float32) * (HEAD_DIM ** -0.5 * LOG2E)
        hi = qs.astype(jnp.bfloat16)
        qt[0:64] = hi
        qt[64:128] = jnp.where(lax.broadcasted_iota(jnp.int32, (64, ROWS), 0) < 2, 1.0, 0.0).astype(jnp.bfloat16)
        qt[128:192] = (qs - hi.astype(jnp.float32)).astype(jnp.bfloat16)
        qt[192:256] = jnp.zeros((64, ROWS), jnp.bfloat16)
        attend_set(qt, blk, kchunk, vchunk, sums, carry, ya, yb, wa, wb)
        for i in range(NT):
            out_local[s, :, i * CH:(i + 1) * CH] = sums[i].astype(jnp.bfloat16)
            carry_out[s, :, i * CH:(i + 1) * CH] = carry[i]
        for p in range(8):
            here = (blk == me) & (t == p)

            @pl.when(jnp.logical_not(here))
            def _():
                piece_copy(s, blk, p).start()

            @pl.when(here)
            def _():
                at[head_rows, :] = out_local[s, :, p * 128:(p + 1) * 128]

        @pl.when(jnp.logical_not(own))
        def _():
            rem_copy(s, blk).start()

        @pl.when(own)
        def _():
            rb[z % 2] = carry_out[s]

        if s == 0:
            for n in range(1, 8):
                remote(fl.at[lanes(0)], fa.at[:, lanes((t - n + 8) % 8)], sf.at[n], sf.at[8 + n], me, t).wait_recv()
            local[6].wait()
            local[7].wait()
            for n in range(8):
                c = slice(n * 256, (n + 1) * 256)
                total[:, c] = jnp.dot(fa[...], fr[:, c], preferred_element_type=jnp.float32)


    for h in range(16):
        hz = h % 4
        column, hcore, _ = query_place(z, x)
        mine = (hz == z) & (column == x) & (2 * (h // 4) + hcore == t)

        @pl.when(jnp.logical_not(mine))
        def _():
            part = at.at[pl.ds(h * 64, 64)]
            remote(part, part, so.at[0, 0], ro.at[h], me, t).wait_recv()
    rows_t = at[...].astype(jnp.float32).T.astype(jnp.bfloat16)
    for n in range(8):
        c = slice(n * 256, (n + 1) * 256)
        mixed[:, c] = (total[:, c] + jnp.dot(rows_t, ar[:, c], preferred_element_type=jnp.float32)).astype(jnp.bfloat16)
    for l in range(2):
        @pl.when(jnp.logical_not(query_local(l)))
        def _():
            remote(rb.at[l], rb.at[l], sr.at[0], rr.at[l], me, t).wait_recv()
        mass[l:l + 1, :] = rb[l, 0:1, :]

    for k in range(NT):
        for c in feature_sends(k):
            c.wait_send()
        relay(k).wait_send()
        for n, sl in enumerate((down, up, far)):
            over(k, n, sl).wait_send()
    for n in range(1, 8):
        filter_copy(n).wait_send()
    for l in range(2):
        @pl.when(2 * core + l != z)
        def _():
            for k in range(NT):
                key_copy(l, k).wait_send()

        @pl.when(jnp.logical_not(query_local(l)))
        def _():
            query_copy(l).wait_send()

    @pl.when(active)
    def _():
        for k in range(NT):
            for zs in range(4):
                pass_on(zs * 4 + x, k, right, xk.at[zs, k, 0]).wait_send()
                pass_on(zs * 4 + x, k, left, xk.at[zs, k, 1]).wait_send()
                pass_on(zs * 4 + x, k, right, fk.at[zs, k]).wait_send()
            for b in range(16):
                pass_on(b, k, me, dk.at[b, k], partner).wait_send()

    for s in range(2):
        blk = set_block(x, core, s)
        own = (blk == me) & (core == z // 2)
        for p in range(8):
            @pl.when(jnp.logical_not((blk == me) & (t == p)))
            def _():
                piece_copy(s, blk, p).wait_send()

        @pl.when(jnp.logical_not(own))
        def _():
            rem_copy(s, blk).wait_send()


def per_device(tokens, norm_gain, signal_proj, postgate_proj, pregate_proj, query_proj, key_proj,
               value_proj, filter_taps, break_bias, filter_readout, attention_readout):
    vmem = pl.BlockSpec(memory_space=pltpu.VMEM)
    hbm = pl.BlockSpec(memory_space=pl.ANY)
    dma = pltpu.SemaphoreType.DMA
    bf16, f32 = jnp.bfloat16, jnp.float32
    mixed, remain = pl.pallas_call(
        layer_kernel,
        out_shape=(jax.ShapeDtypeStruct((128, 2048), bf16), jax.ShapeDtypeStruct((2, ROWS), f32)),
        in_specs=[vmem, vmem] + [hbm] * 6 + [vmem, vmem, hbm, hbm],
        out_specs=(vmem, vmem),
        scratch_shapes=[
            pltpu.VMEM((8, ROWS, 256), bf16),
            pltpu.VMEM((2048, 768), bf16),
            pltpu.VMEM((1024, 2048), bf16),
            pltpu.VMEM((1024, 2048), bf16),
            pltpu.VMEM((CH, 2048), bf16),
            pltpu.VMEM((ROWS + 8, 128), f32),
            pltpu.VMEM((ROWS, 128), bf16),
            pltpu.VMEM((ROWS, 128), bf16),
            pltpu.VMEM((128, ROWS), bf16),
            pltpu.VMEM((2, NT, 384, 128), bf16),
            pltpu.VMEM((16, NT, 384, 128), bf16),
            pltpu.VMEM((2, 64, ROWS), bf16),
            pltpu.VMEM((2, 8, ROWS), f32),
            pltpu.VMEM((128, 1024), bf16),
            pltpu.VMEM((1024, 128), bf16),
            pltpu.VMEM((128, 2048), f32),
            pltpu.VMEM((256, ROWS), bf16),
            pltpu.VMEM((2, 64, ROWS), bf16),
            pltpu.VMEM((2, 8, ROWS), f32),
            pltpu.VMEM((NT, 64, CH), f32),
            pltpu.VMEM((NT, 8, CH), f32),
            pltpu.VMEM((NT, CH, CH), f32),
            pltpu.VMEM((NT, CH, CH), f32),
            pltpu.VMEM((NT, CH, CH), bf16),
            pltpu.VMEM((NT, CH, CH), bf16),
            dma((8,)), dma((4, 8)), dma((8, 4)), dma((16,)), dma((2,)),
            dma((16, 4)), dma((2,)), dma((16,)), dma((2,)),
            dma((2, 4)), dma((2,)), dma((2, 8)), dma((2,)),
            dma((4, 4, 2)), dma((16, 4)), dma((4, 4)),
        ],
        compiler_params=pltpu.CompilerParams(vmem_limit_bytes=60 * 2**20, has_side_effects=True, collective_id=0),
    )(tokens, norm_gain.reshape(1, -1), signal_proj, postgate_proj, pregate_proj, query_proj, key_proj,
      value_proj, filter_taps, break_bias.T, filter_readout, attention_readout)
    return mixed, jnp.log(jnp.maximum(1.0 - remain, mass_floor))


def solution(mesh):
    placed = (P("sp", "tp"), P()) + (P(None, "tp"),) * 7 + (P("sp", "tp"), P(), P())
    return jax.shard_map(per_device, mesh=mesh, in_specs=placed,
                         out_specs=(P(("sp", "tp"), None), P("tp", "sp")), check_vma=False)
```

```python
import jax
import jax.numpy as jnp
from jax import lax
from jax.experimental import pallas as pl
from jax.experimental.pallas import tpu as pltpu
from jax.sharding import PartitionSpec as P

HEAD_DIM = 64
CONV_W = 3
CH = 256
NT = 4
CAP = 24.0
QROWS = 256
LOG2E = 1.4426950408889634
epsilon = 1e-06
mass_floor = 0.1


def scan_chunk(y_ref, carry_ref, w_ref, masked):
    seg = CH // 8
    if masked:
        row = lax.broadcasted_iota(jnp.int32, (8, CH), 0) * seg
        col = lax.broadcasted_iota(jnp.int32, (8, CH), 1)
        diff = col - row
    r = jnp.ones((8, CH), jnp.float32)
    for g in reversed(range(seg // 4)):
        us, ds = [], []
        for k in range(4):
            j = 4 * g + k
            u = jnp.exp2(jnp.minimum(y_ref[j * 8:(j + 1) * 8, :], CAP))
            if masked:
                u = jnp.where(diff > j, u, 0.0)
            us.append(u)
            ds.append(1.0 + u)
        low, high = ds[0] * ds[1], ds[2] * ds[3]
        r = r * (1.0 / (low * high))
        e = r * low
        ws = [us[0] * r, us[1] * (r * ds[0]), us[2] * e, us[3] * (e * ds[2])]
        for k in (0, 2):
            j = 4 * g + k
            w_ref[j * 8:(j + 2) * 8, :] = jnp.concatenate(ws[k:k + 2], axis=0).astype(jnp.bfloat16)
    sub = lax.broadcasted_iota(jnp.int32, (8, CH), 0)
    s = r
    for k in (1, 2, 4):
        s = s * jnp.where(sub < 8 - k, pltpu.roll(s, 8 - k, 0), 1.0)
    carry = carry_ref[...]
    c = jnp.where(sub < 7, pltpu.roll(s, 7, 0), 1.0) * carry
    carry_ref[...] = carry * jnp.broadcast_to(s[0:1, :], (8, CH))
    c = jnp.concatenate([c, c], axis=0).astype(jnp.bfloat16)
    for j in range(CH // 16):
        w_ref[j * 16:(j + 1) * 16, :] = w_ref[j * 16:(j + 1) * 16, :] * c

def scores_to(y_ref, kk, q_ref, tile):
    lhs = jnp.concatenate([kk, kk], axis=1)
    rhs = q_ref[:, tile * CH:(tile + 1) * CH]
    for i in range(0, CH, QROWS):
        y_ref[i:i + QROWS, :] = jnp.dot(lhs[i:i + QROWS], rhs, preferred_element_type=jnp.float32)

def attend_set(qt, blk, kchunk, vchunk, acc, carry, ya, yb, wa, wb):
    base = 4 * blk
    for t in range(NT):
        acc[t] = jnp.zeros_like(acc[t])
        carry[t] = jnp.ones((8, CH), jnp.float32)
    for c in reversed(range(NT)):
        kk = kchunk(base + c)
        for t in range(c, NT):
            scores_to(ya.at[t], kk, qt, t)
        for t in range(c, NT):
            scan_chunk(ya.at[t], carry.at[t], wb.at[t], t == c)
        if c > 0:
            vv = vchunk(base + c)
            for t in range(c, NT):
                acc[t] += jnp.dot(vv, wb[t], preferred_element_type=jnp.float32)
    kk = kchunk(jnp.maximum(base - 1, 0))
    for t in range(NT):
        scores_to(ya.at[t], kk, qt, t)

    def half(c, ysrc, ydst, wdst, wsrc):
        kn = kchunk(jnp.maximum(c - 1, 0))
        vp = vchunk(c + 1)
        for t in range(NT):
            scan_chunk(ysrc.at[t], carry.at[t], wdst.at[t], False)
            scores_to(ydst.at[t], kn, qt, t)
            acc[t] += jnp.dot(vp, wsrc[t], preferred_element_type=jnp.float32)

    def body(p, _):
        c = base - 1 - 2 * p
        half(c, ya, yb, wa, wb)
        half(c - 1, yb, ya, wb, wa)
        return 0
    lax.fori_loop(0, 2 * blk, body, 0)
    vp = vchunk(0)
    for t in range(NT):
        acc[t] += jnp.dot(vp, wb[t], preferred_element_type=jnp.float32)


SP, TP = "sp", "tp"
ROWS = NT * CH


def remote(src, dst, send, recv, sp, tp):
    return pltpu.make_async_remote_copy(src_ref=src, dst_ref=dst, send_sem=send, recv_sem=recv,
                                        device_id={SP: sp, TP: tp}, device_id_type=pl.DeviceIdType.MESH)


def query_place(z, x):
    column = jnp.where((z == 1) | (z == 3), 3 - x, x)
    core = jnp.where((z == 1) | (z == 2), 1, 0)
    slot = jnp.where((z == 2) | (z == 3), 0, 1)
    return column, core, slot


def set_block(x, core, slot):
    return jnp.where(core == 0, jnp.where(slot == 0, 15 - x, x), jnp.where(slot == 0, 8 + x, 7 - x))


def layer_kernel(tokens, gain, w0, w1, w2, w3, w4, w5, taps, bias, fr_hbm, ar_hbm, mixed, mass,
                 tk, wts, fr, ar, sc, pr, post, fl, q, kvp, kvb, kx, qb, rb, fa, at, total,
                 qt, out_local, carry_out, sums, carry, ya, yb, wa, wb,
                 lw, st, rt, sf, rim,
                 rk, rq, ro, rr, sk, sq, so, sr, xk, dk, fk):
    me = lax.axis_index(SP)
    t = lax.axis_index(TP)
    z, x = me // 4, me % 4
    core = t % 2
    y = t // 2
    partner = t + 1 - 2 * core
    active = core == z // 2
    right = z * 4 + (x + 1) % 4
    left = z * 4 + (x + 3) % 4

    back = t - core + z // 2
    col, qcore, slot = query_place(z, x)
    qtp = t - core + qcore

    def query_local(l):
        return (2 * core + l == z) & (col == x) & (qcore == core)

    barrier = pltpu.get_barrier_semaphore()

    def greet(sp, tp):
        pl.semaphore_signal(barrier, inc=1, device_id={SP: sp, TP: tp}, device_id_type=pl.DeviceIdType.MESH)

    for n in range(1, 8):
        greet(me, (t + n) % 8)
    greet(right, t)
    greet(left, t)
    for n in range(1, 4):
        greet((me + 4 * n) % 16, t)
    expected = 12
    for s in range(2):
        blk = set_block(x, core, s)

        @pl.when(jnp.logical_not((blk == me) & (core == z // 2)))
        def _():
            greet(blk, back)
        expected = expected + jnp.where(query_local(s), 0, 1)

    @pl.when(me > 0)
    def _():
        greet(me - 1, t)
    expected = expected + jnp.where(me < 15, 1, 0)

    local = [pltpu.make_async_copy(w, wts.at[:, i * 128:(i + 1) * 128], lw.at[i])
             for i, w in enumerate((w0, w1, w2, w3, w4, w5))]
    local += [pltpu.make_async_copy(fr_hbm, fr, lw.at[6]), pltpu.make_async_copy(ar_hbm, ar, lw.at[7])]

    up = (t + 2) % 8
    down = (t + 6) % 8
    far = (t + 4) % 8

    def rows(k):
        return pl.ds(k * CH, CH)

    def feature_sends(k):
        src = tokens.at[rows(k)]
        dst = tk.at[t, rows(k)]
        return [remote(src, dst, st.at[k, 0], rt.at[t, k], me, up),
                remote(src, dst, st.at[k, 1], rt.at[t, k], me, down),
                remote(src, dst, st.at[k, 2], rt.at[t, k], me, partner)]

    def relay(k):
        slot, to = (down, up) if k % 2 == 0 else (up, down)
        part = tk.at[slot, rows(k)]
        return remote(part, part, st.at[k, 3], rt.at[slot, k], me, to)

    def over(k, n, slot):
        part = tk.at[slot, rows(k)]
        return remote(part, part, st.at[k, 4 + n], rt.at[slot, k], me, partner)

    def got(slot, k):
        part = tk.at[slot, rows(k)]
        remote(part, part, st.at[k, 0], rt.at[slot, k], me, t).wait_recv()

    def near(k):
        got(down, k)
        got(up, k)
        relay(k).start()
        over(k, 0, down).start()
        over(k, 1, up).start()
        if k + 2 < NT:
            for c in feature_sends(k + 2):
                c.start()

    def rest(k):
        got(far, k)
        over(k, 2, far).start()
        for n in (0, 2, 4, 6):
            got((partner + n) % 8, k)

    rowi = lax.broadcasted_iota(jnp.int32, (CH, CH), 0)
    coli = lax.broadcasted_iota(jnp.int32, (CH, CH), 1)
    order = jnp.where(coli == (rowi % 8) * (CH // 8) + rowi // 8, 1.0, 0.0).astype(jnp.bfloat16)
    half = lax.broadcasted_iota(jnp.int32, (128, 128), 1) < 64

    def project(k):
        r = rows(k)
        squares = jnp.zeros((CH, 128), jnp.float32)
        for s in range(8):
            v = tk[s, r, :].astype(jnp.float32)
            v2 = v * v
            squares = squares + v2[:, :128] + v2[:, 128:]
            sc[:, s * 256:(s + 1) * 256] = (v * gain[:, s * 256:(s + 1) * 256]).astype(jnp.bfloat16)
        inverse = lax.rsqrt(jnp.sum(squares, axis=1, keepdims=True) * (1.0 / 2048.0) + epsilon)

        def product(n):
            p = jnp.dot(sc[...], wts[:, n * 256:(n + 1) * 256], preferred_element_type=jnp.float32)
            p = (p * inverse).astype(jnp.bfloat16)
            return p[:, :128], p[:, 128:]

        signal, post_gate = product(0)
        pre_gate, queries = product(1)
        keys, values = product(2)
        pr[8 + k * CH:8 + (k + 1) * CH, :] = pre_gate.astype(jnp.float32) * signal.astype(jnp.float32)
        post[r, :] = post_gate
        q[:, r] = queries.astype(jnp.float32).T.astype(jnp.bfloat16)
        b = bias[:, r].astype(jnp.float32) * LOG2E
        hi = b.astype(jnp.bfloat16).astype(jnp.float32)
        four = jnp.concatenate([hi[0:1], (b - hi)[0:1], hi[1:2], (b - hi)[1:2], jnp.zeros((4, CH), jnp.float32)], axis=0)
        four = lax.dot_general(four.astype(jnp.bfloat16), order, (((1,), (1,)), ((), ())),
                               preferred_element_type=jnp.float32)
        four = jnp.concatenate([four[:, :128], four[:, 128:]], axis=0).astype(jnp.bfloat16)
        kk = jnp.dot(order, keys, preferred_element_type=jnp.float32)
        top, bottom = kk[:128], kk[128:]
        packed = (jnp.where(half, top, pltpu.roll(bottom, 64, 1)), jnp.where(half, pltpu.roll(top, 64, 1), bottom))
        vv = jnp.dot(order, values, preferred_element_type=jnp.float32).T.astype(jnp.bfloat16)
        for l in range(2):
            kvp[l, k, 0:128, :] = packed[l].astype(jnp.bfloat16)
            kvp[l, k, 128:192, :] = vv[l * 64:(l + 1) * 64, :128]
            kvp[l, k, 192:256, :] = vv[l * 64:(l + 1) * 64, 128:]
            kvp[l, k, 256:272, :] = four

    for c in local:
        c.start()
    tk[t] = tokens[...]
    pl.semaphore_wait(barrier, expected)
    for k in range(2):
        for c in feature_sends(k):
            c.start()


    def key_copy(l, k):
        g = 2 * core + l
        return remote(kvp.at[l, k], kvb.at[me, k], sk.at[l, k], rk.at[me, k], g * 4 + x, t)

    def send_keys(k):
        for l in range(2):
            @pl.when(2 * core + l != z)
            def _():
                key_copy(l, k).start()

            @pl.when(2 * core + l == z)
            def _():
                kvb[me, k] = kvp[l, k]

    def pass_on(b, k, to, sem, tp=t, src=None):
        return remote(kvb.at[b, k] if src is None else src, kvb.at[b, k], sem, rk.at[b, k], to, tp)

    def arrived(b, k):
        pass_on(b, k, me, sk.at[0, 0]).wait_recv()

    def own_column(k):
        @pl.when(active)
        def _():
            for zs in range(4):
                b = zs * 4 + x

                def spread(src):
                    pass_on(b, k, right, xk.at[zs, k, 0], src=src).start()
                    pass_on(b, k, left, xk.at[zs, k, 1], src=src).start()
                    pass_on(b, k, me, dk.at[b, k], partner, src=src).start()

                @pl.when(z != zs)
                def _():
                    arrived(b, k)
                    spread(None)

                @pl.when(z == zs)
                def _():
                    spread(kvp.at[zs % 2, k])

    def near_columns(k):
        @pl.when(active)
        def _():
            for zs in range(4):
                even = (zs + k) % 2 == 0
                b = zs * 4 + (x + 3) % 4
                arrived(b, k)
                if even:
                    pass_on(b, k, right, fk.at[zs, k]).start()
                pass_on(b, k, me, dk.at[b, k], partner).start()
                b = zs * 4 + (x + 1) % 4
                arrived(b, k)
                if not even:
                    pass_on(b, k, left, fk.at[zs, k]).start()
                pass_on(b, k, me, dk.at[b, k], partner).start()

    def far_column(k):
        @pl.when(active)
        def _():
            for zs in range(4):
                b = zs * 4 + (x + 2) % 4
                arrived(b, k)
                pass_on(b, k, me, dk.at[b, k], partner).start()

    brow = lax.broadcasted_iota(jnp.int32, (16, 256), 0)
    bcol = lax.broadcasted_iota(jnp.int32, (16, 256), 1)
    bpart = bcol % 128 - 64
    select = jnp.where((bpart >= 0) & (bpart < 2) & (brow == (bcol // 128) * 8 + 2 * (z % 2) + bpart), 1.0, 0.0)
    select = select.astype(jnp.bfloat16)

    def unpack(k):
        def four(n, _):
            for i in range(4):
                b = 4 * n + i
                packed = kvb[b, k, 0:128, :].astype(jnp.float32)
                extra = lax.dot_general(kvb[b, k, 256:272, :], select, (((0,), (0,)), ((), ())),
                                        preferred_element_type=jnp.float32)
                kx[b, k, 0:128, :] = jnp.where(half, packed, extra[:, :128]).astype(jnp.bfloat16)
                kx[b, k, 128:256, :] = jnp.where(half, pltpu.roll(packed, 64, 1), extra[:, 128:]).astype(jnp.bfloat16)
            return 0
        lax.fori_loop(0, 4, four, 0)

    def passive_arrivals(k):
        @pl.when(jnp.logical_not(active))
        def _():
            for b in range(16):
                arrived(b, k)

    near(0)
    near(1)
    rest(0)
    for c in local[:6]:
        c.wait()
    project(0)
    send_keys(0)
    near(2)
    rest(1)
    project(1)
    send_keys(1)
    own_column(0)
    near(3)
    rest(2)
    project(2)
    send_keys(2)
    own_column(1)
    near_columns(0)
    rest(3)
    project(3)
    send_keys(3)

    def query_copy(l):
        g = 2 * core + l
        return remote(q.at[pl.ds(l * 64, 64)], qb.at[slot], sq.at[l], rq.at[slot], g * 4 + col, qtp)

    for l in range(2):
        @pl.when(jnp.logical_not(query_local(l)))
        def _():
            query_copy(l).start()

        @pl.when(query_local(l))
        def _():
            qb[slot] = q[l * 64:(l + 1) * 64, :]

    def rim_copy():
        return remote(pr.at[pl.ds(ROWS, 8)], pr.at[pl.ds(0, 8)], rim.at[0], rim.at[1], (me + 1) % 16, t)

    @pl.when(me < 15)
    def _():
        rim_copy().start()

    own_column(2)
    near_columns(1)
    far_column(0)
    own_column(3)
    near_columns(2)
    far_column(1)

    @pl.when(me == 0)
    def _():
        pr[0:8, :] = jnp.zeros((8, 128), jnp.float32)

    @pl.when(me > 0)
    def _():
        rim_copy().wait_recv()
    tp_values = taps[...].astype(jnp.float32)
    running = jnp.zeros((ROWS, 128), jnp.float32)
    for w in range(CONV_W):
        running = running + tp_values[w:w + 1, :] * pr[6 + w:6 + w + ROWS, :]
    fl[...] = (post[...].astype(jnp.float32) * running).astype(jnp.bfloat16)

    @pl.when(me < 15)
    def _():
        rim_copy().wait_send()

    def lanes(i):
        return pl.ds(pl.multiple_of(i * 128, 128), 128)

    def filter_copy(n):
        p = (t + n) % 8
        return remote(fl.at[lanes(p)], fa.at[:, lanes(t)], sf.at[n], sf.at[8 + n], me, p)

    for n in range(1, 8):
        filter_copy(n).start()
    fa[:, lanes(t)] = fl[lanes(t), :]

    near_columns(3)
    passive_arrivals(0)
    unpack(0)
    passive_arrivals(1)
    unpack(1)
    far_column(2)
    passive_arrivals(2)
    unpack(2)
    far_column(3)
    passive_arrivals(3)
    unpack(3)

    def kchunk(c):
        return kx[c // NT, c % NT]

    def vchunk(c):
        return jnp.concatenate([kvb[c // NT, c % NT, 128:192, :], kvb[c // NT, c % NT, 192:256, :]], axis=1)

    head_rows = pl.ds(pl.multiple_of((4 * y + z) * 64, 64), 64)

    def piece_copy(s, blk, p):
        return remote(out_local.at[s, :, pl.ds(p * 128, 128)], at.at[head_rows], so.at[s, p],
                      ro.at[4 * y + z], blk, p)

    def rem_copy(s, blk):
        return remote(carry_out.at[s], rb.at[z % 2], sr.at[s], rr.at[z % 2], blk, back)

    for s in range(2):
        blk = set_block(x, core, s)
        own = (blk == me) & (core == z // 2)

        @pl.when(jnp.logical_not(own))
        def _():
            remote(qb.at[s], qb.at[s], sq.at[0], rq.at[s], me, t).wait_recv()
        qs = qb[s].astype(jnp.float32) * (HEAD_DIM ** -0.5 * LOG2E)
        hi = qs.astype(jnp.bfloat16)
        qt[0:64] = hi
        qt[64:128] = jnp.where(lax.broadcasted_iota(jnp.int32, (64, ROWS), 0) < 2, 1.0, 0.0).astype(jnp.bfloat16)
        qt[128:192] = (qs - hi.astype(jnp.float32)).astype(jnp.bfloat16)
        qt[192:256] = jnp.zeros((64, ROWS), jnp.bfloat16)
        attend_set(qt, blk, kchunk, vchunk, sums, carry, ya, yb, wa, wb)
        for i in range(NT):
            out_local[s, :, i * CH:(i + 1) * CH] = sums[i].astype(jnp.bfloat16)
            carry_out[s, :, i * CH:(i + 1) * CH] = carry[i]
        for p in range(8):
            here = (blk == me) & (t == p)

            @pl.when(jnp.logical_not(here))
            def _():
                piece_copy(s, blk, p).start()

            @pl.when(here)
            def _():
                at[head_rows, :] = out_local[s, :, p * 128:(p + 1) * 128]

        @pl.when(jnp.logical_not(own))
        def _():
            rem_copy(s, blk).start()

        @pl.when(own)
        def _():
            rb[z % 2] = carry_out[s]

        if s == 0:
            for n in range(1, 8):
                remote(fl.at[lanes(0)], fa.at[:, lanes((t - n + 8) % 8)], sf.at[n], sf.at[8 + n], me, t).wait_recv()
            local[6].wait()
            local[7].wait()
            for n in range(8):
                c = slice(n * 256, (n + 1) * 256)
                total[:, c] = jnp.dot(fa[...], fr[:, c], preferred_element_type=jnp.float32)


    for h in range(16):
        hz = h % 4
        column, hcore, _ = query_place(z, x)
        mine = (hz == z) & (column == x) & (2 * (h // 4) + hcore == t)

        @pl.when(jnp.logical_not(mine))
        def _():
            part = at.at[pl.ds(h * 64, 64)]
            remote(part, part, so.at[0, 0], ro.at[h], me, t).wait_recv()
    rows_t = at[...].astype(jnp.float32).T.astype(jnp.bfloat16)
    for n in range(8):
        c = slice(n * 256, (n + 1) * 256)
        mixed[:, c] = (total[:, c] + jnp.dot(rows_t, ar[:, c], preferred_element_type=jnp.float32)).astype(jnp.bfloat16)
    for l in range(2):
        @pl.when(jnp.logical_not(query_local(l)))
        def _():
            remote(rb.at[l], rb.at[l], sr.at[0], rr.at[l], me, t).wait_recv()
        mass[l:l + 1, :] = rb[l, 0:1, :]

    for k in range(NT):
        for c in feature_sends(k):
            c.wait_send()
        relay(k).wait_send()
        for n, sl in enumerate((down, up, far)):
            over(k, n, sl).wait_send()
    for n in range(1, 8):
        filter_copy(n).wait_send()
    for l in range(2):
        @pl.when(2 * core + l != z)
        def _():
            for k in range(NT):
                key_copy(l, k).wait_send()

        @pl.when(jnp.logical_not(query_local(l)))
        def _():
            query_copy(l).wait_send()

    @pl.when(active)
    def _():
        for k in range(NT):
            for zs in range(4):
                pass_on(zs * 4 + x, k, right, xk.at[zs, k, 0]).wait_send()
                pass_on(zs * 4 + x, k, left, xk.at[zs, k, 1]).wait_send()
                pass_on(zs * 4 + x, k, right, fk.at[zs, k]).wait_send()
            for b in range(16):
                pass_on(b, k, me, dk.at[b, k], partner).wait_send()

    for s in range(2):
        blk = set_block(x, core, s)
        own = (blk == me) & (core == z // 2)
        for p in range(8):
            @pl.when(jnp.logical_not((blk == me) & (t == p)))
            def _():
                piece_copy(s, blk, p).wait_send()

        @pl.when(jnp.logical_not(own))
        def _():
            rem_copy(s, blk).wait_send()


def per_device(tokens, norm_gain, signal_proj, postgate_proj, pregate_proj, query_proj, key_proj,
               value_proj, filter_taps, break_bias, filter_readout, attention_readout):
    vmem = pl.BlockSpec(memory_space=pltpu.VMEM)
    hbm = pl.BlockSpec(memory_space=pl.ANY)
    dma = pltpu.SemaphoreType.DMA
    bf16, f32 = jnp.bfloat16, jnp.float32
    mixed, remain = pl.pallas_call(
        layer_kernel,
        out_shape=(jax.ShapeDtypeStruct((128, 2048), bf16), jax.ShapeDtypeStruct((2, ROWS), f32)),
        in_specs=[vmem, vmem] + [hbm] * 6 + [vmem, vmem, hbm, hbm],
        out_specs=(vmem, vmem),
        scratch_shapes=[
            pltpu.VMEM((8, ROWS, 256), bf16),
            pltpu.VMEM((2048, 768), bf16),
            pltpu.VMEM((1024, 2048), bf16),
            pltpu.VMEM((1024, 2048), bf16),
            pltpu.VMEM((CH, 2048), bf16),
            pltpu.VMEM((ROWS + 8, 128), f32),
            pltpu.VMEM((ROWS, 128), bf16),
            pltpu.VMEM((ROWS, 128), bf16),
            pltpu.VMEM((128, ROWS), bf16),
            pltpu.VMEM((2, NT, 272, 128), bf16),
            pltpu.VMEM((16, NT, 272, 128), bf16),
            pltpu.VMEM((16, NT, CH, 128), bf16),
            pltpu.VMEM((2, 64, ROWS), bf16),
            pltpu.VMEM((2, 8, ROWS), f32),
            pltpu.VMEM((128, 1024), bf16),
            pltpu.VMEM((1024, 128), bf16),
            pltpu.VMEM((128, 2048), f32),
            pltpu.VMEM((256, ROWS), bf16),
            pltpu.VMEM((2, 64, ROWS), bf16),
            pltpu.VMEM((2, 8, ROWS), f32),
            pltpu.VMEM((NT, 64, CH), f32),
            pltpu.VMEM((NT, 8, CH), f32),
            pltpu.VMEM((NT, CH, CH), f32),
            pltpu.VMEM((NT, CH, CH), f32),
            pltpu.VMEM((NT, CH, CH), bf16),
            pltpu.VMEM((NT, CH, CH), bf16),
            dma((8,)), dma((4, 8)), dma((8, 4)), dma((16,)), dma((2,)),
            dma((16, 4)), dma((2,)), dma((16,)), dma((2,)),
            dma((2, 4)), dma((2,)), dma((2, 8)), dma((2,)),
            dma((4, 4, 2)), dma((16, 4)), dma((4, 4)),
        ],
        compiler_params=pltpu.CompilerParams(vmem_limit_bytes=60 * 2**20, has_side_effects=True, collective_id=0),
    )(tokens, norm_gain.reshape(1, -1), signal_proj, postgate_proj, pregate_proj, query_proj, key_proj,
      value_proj, filter_taps, break_bias.T, filter_readout, attention_readout)
    return mixed, jnp.log(jnp.maximum(1.0 - remain, mass_floor))


def solution(mesh):
    placed = (P("sp", "tp"), P()) + (P(None, "tp"),) * 7 + (P("sp", "tp"), P(), P())
    return jax.shard_map(per_device, mesh=mesh, in_specs=placed,
                         out_specs=(P(("sp", "tp"), None), P("tp", "sp")), check_vma=False)
```

```python
import jax
import jax.numpy as jnp
from jax import lax
from jax.experimental import pallas as pl
from jax.experimental.pallas import tpu as pltpu
from jax.sharding import PartitionSpec as P

HEAD_DIM = 64
CONV_W = 3
CH = 256
NT = 4
CAP = 24.0
QROWS = 256
LOG2E = 1.4426950408889634
epsilon = 1e-06
mass_floor = 0.1


def scan_chunk(y_ref, carry_ref, w_ref, masked):
    seg = CH // 8
    if masked:
        row = lax.broadcasted_iota(jnp.int32, (8, CH), 0) * seg
        col = lax.broadcasted_iota(jnp.int32, (8, CH), 1)
        diff = col - row
    r = jnp.ones((8, CH), jnp.float32)
    for g in reversed(range(seg // 4)):
        us, ds = [], []
        for k in range(4):
            j = 4 * g + k
            u = jnp.exp2(jnp.minimum(y_ref[j * 8:(j + 1) * 8, :], CAP))
            if masked:
                u = jnp.where(diff > j, u, 0.0)
            us.append(u)
            ds.append(1.0 + u)
        low, high = ds[0] * ds[1], ds[2] * ds[3]
        r = r * (1.0 / (low * high))
        e = r * low
        ws = [us[0] * r, us[1] * (r * ds[0]), us[2] * e, us[3] * (e * ds[2])]
        for k in (0, 2):
            j = 4 * g + k
            w_ref[j * 8:(j + 2) * 8, :] = jnp.concatenate(ws[k:k + 2], axis=0).astype(jnp.bfloat16)
    sub = lax.broadcasted_iota(jnp.int32, (8, CH), 0)
    s = r
    for k in (1, 2, 4):
        s = s * jnp.where(sub < 8 - k, pltpu.roll(s, 8 - k, 0), 1.0)
    carry = carry_ref[...]
    c = jnp.where(sub < 7, pltpu.roll(s, 7, 0), 1.0) * carry
    carry_ref[...] = carry * jnp.broadcast_to(s[0:1, :], (8, CH))
    c = jnp.concatenate([c, c], axis=0).astype(jnp.bfloat16)
    for j in range(CH // 16):
        w_ref[j * 16:(j + 1) * 16, :] = w_ref[j * 16:(j + 1) * 16, :] * c

def scores_to(y_ref, kk, q_ref, tile):
    lhs = jnp.concatenate([kk, kk], axis=1)
    rhs = q_ref[:, tile * CH:(tile + 1) * CH]
    for i in range(0, CH, QROWS):
        y_ref[i:i + QROWS, :] = jnp.dot(lhs[i:i + QROWS], rhs, preferred_element_type=jnp.float32)

def attend_own(qt, blk, kchunk, vchunk, acc, carry, ya, wb):
    base = 4 * blk
    for t in range(NT):
        acc[t] = jnp.zeros_like(acc[t])
        carry[t] = jnp.ones((8, CH), jnp.float32)
    for c in reversed(range(NT)):
        kk = kchunk(base + c)
        for t in range(c, NT):
            scores_to(ya.at[t], kk, qt, t)
        for t in range(c, NT):
            scan_chunk(ya.at[t], carry.at[t], wb.at[t], t == c)
        if c > 0:
            vv = vchunk(base + c)
            for t in range(c, NT):
                acc[t] += jnp.dot(vv, wb[t], preferred_element_type=jnp.float32)


def attend_before(qt, blk, kchunk, vchunk, acc, carry, ya, yb, wa, wb):
    base = 4 * blk
    kk = kchunk(jnp.maximum(base - 1, 0))
    for t in range(NT):
        scores_to(ya.at[t], kk, qt, t)

    def half(c, ysrc, ydst, wdst, wsrc):
        kn = kchunk(jnp.maximum(c - 1, 0))
        vp = vchunk(c + 1)
        for t in range(NT):
            scan_chunk(ysrc.at[t], carry.at[t], wdst.at[t], False)
            scores_to(ydst.at[t], kn, qt, t)
            acc[t] += jnp.dot(vp, wsrc[t], preferred_element_type=jnp.float32)

    def body(p, _):
        c = base - 1 - 2 * p
        half(c, ya, yb, wa, wb)
        half(c - 1, yb, ya, wb, wa)
        return 0
    lax.fori_loop(0, 2 * blk, body, 0)
    vp = vchunk(0)
    for t in range(NT):
        acc[t] += jnp.dot(vp, wb[t], preferred_element_type=jnp.float32)


SP, TP = "sp", "tp"
ROWS = NT * CH


def remote(src, dst, send, recv, sp, tp):
    return pltpu.make_async_remote_copy(src_ref=src, dst_ref=dst, send_sem=send, recv_sem=recv,
                                        device_id={SP: sp, TP: tp}, device_id_type=pl.DeviceIdType.MESH)


def query_place(z, x):
    column = jnp.where((z == 1) | (z == 3), 3 - x, x)
    core = jnp.where((z == 1) | (z == 2), 1, 0)
    slot = jnp.where((z == 2) | (z == 3), 0, 1)
    return column, core, slot


def set_block(x, core, slot):
    return jnp.where(core == 0, jnp.where(slot == 0, 15 - x, x), jnp.where(slot == 0, 8 + x, 7 - x))


def layer_kernel(tokens, gain, w0, w1, w2, w3, w4, w5, taps, bias, fr_hbm, ar_hbm, mixed, mass,
                 tk, wts, fr, ar, sc, pr, post, fl, q, kvp, kvb, kx, qb, rb, fa, at, total,
                 qt, out_local, carry_out, sums, carry, ya, yb, wa, wb,
                 lw, st, rt, sf, rim,
                 rk, rq, ro, rr, sk, sq, so, sr, xk, dk, fk):
    me = lax.axis_index(SP)
    t = lax.axis_index(TP)
    z, x = me // 4, me % 4
    core = t % 2
    y = t // 2
    partner = t + 1 - 2 * core
    active = core == z // 2
    right = z * 4 + (x + 1) % 4
    left = z * 4 + (x + 3) % 4

    back = t - core + z // 2
    col, qcore, slot = query_place(z, x)
    qtp = t - core + qcore

    def query_local(l):
        return (2 * core + l == z) & (col == x) & (qcore == core)

    barrier = pltpu.get_barrier_semaphore()

    def greet(sp, tp):
        pl.semaphore_signal(barrier, inc=1, device_id={SP: sp, TP: tp}, device_id_type=pl.DeviceIdType.MESH)

    for n in range(1, 8):
        greet(me, (t + n) % 8)
    greet(right, t)
    greet(left, t)
    for n in range(1, 4):
        greet((me + 4 * n) % 16, t)
    expected = 12
    for s in range(2):
        blk = set_block(x, core, s)

        @pl.when(jnp.logical_not((blk == me) & (core == z // 2)))
        def _():
            greet(blk, back)
        expected = expected + jnp.where(query_local(s), 0, 1)

    @pl.when(me > 0)
    def _():
        greet(me - 1, t)
    expected = expected + jnp.where(me < 15, 1, 0)

    local = [pltpu.make_async_copy(w, wts.at[:, i * 128:(i + 1) * 128], lw.at[i])
             for i, w in enumerate((w0, w1, w2, w3, w4, w5))]
    local += [pltpu.make_async_copy(fr_hbm, fr, lw.at[6]), pltpu.make_async_copy(ar_hbm, ar, lw.at[7])]

    up = (t + 2) % 8
    down = (t + 6) % 8
    far = (t + 4) % 8

    def rows(k):
        return pl.ds(k * CH, CH)

    def feature_sends(k):
        src = tokens.at[rows(k)]
        dst = tk.at[t, rows(k)]
        return [remote(src, dst, st.at[k, 0], rt.at[t, k], me, up),
                remote(src, dst, st.at[k, 1], rt.at[t, k], me, down),
                remote(src, dst, st.at[k, 2], rt.at[t, k], me, partner)]

    def relay(k):
        slot, to = (down, up) if k % 2 == 0 else (up, down)
        part = tk.at[slot, rows(k)]
        return remote(part, part, st.at[k, 3], rt.at[slot, k], me, to)

    def over(k, n, slot):
        part = tk.at[slot, rows(k)]
        return remote(part, part, st.at[k, 4 + n], rt.at[slot, k], me, partner)

    def got(slot, k):
        part = tk.at[slot, rows(k)]
        remote(part, part, st.at[k, 0], rt.at[slot, k], me, t).wait_recv()

    def near(k):
        got(down, k)
        got(up, k)
        relay(k).start()
        over(k, 0, down).start()
        over(k, 1, up).start()
        if k + 2 < NT:
            for c in feature_sends(k + 2):
                c.start()

    def rest(k):
        got(far, k)
        over(k, 2, far).start()
        for n in (0, 2, 4, 6):
            got((partner + n) % 8, k)

    rowi = lax.broadcasted_iota(jnp.int32, (CH, CH), 0)
    coli = lax.broadcasted_iota(jnp.int32, (CH, CH), 1)
    order = jnp.where(coli == (rowi % 8) * (CH // 8) + rowi // 8, 1.0, 0.0).astype(jnp.bfloat16)
    half = lax.broadcasted_iota(jnp.int32, (128, 128), 1) < 64

    def project(k):
        r = rows(k)
        squares = jnp.zeros((CH, 128), jnp.float32)
        for s in range(8):
            v = tk[s, r, :].astype(jnp.float32)
            v2 = v * v
            squares = squares + v2[:, :128] + v2[:, 128:]
            sc[:, s * 256:(s + 1) * 256] = (v * gain[:, s * 256:(s + 1) * 256]).astype(jnp.bfloat16)
        inverse = lax.rsqrt(jnp.sum(squares, axis=1, keepdims=True) * (1.0 / 2048.0) + epsilon)

        def product(n):
            p = jnp.dot(sc[...], wts[:, n * 256:(n + 1) * 256], preferred_element_type=jnp.float32)
            p = (p * inverse).astype(jnp.bfloat16)
            return p[:, :128], p[:, 128:]

        signal, post_gate = product(0)
        pre_gate, queries = product(1)
        keys, values = product(2)
        pr[8 + k * CH:8 + (k + 1) * CH, :] = pre_gate.astype(jnp.float32) * signal.astype(jnp.float32)
        post[r, :] = post_gate
        q[:, r] = queries.astype(jnp.float32).T.astype(jnp.bfloat16)
        b = bias[:, r].astype(jnp.float32) * LOG2E
        hi = b.astype(jnp.bfloat16).astype(jnp.float32)
        four = jnp.concatenate([hi[0:1], (b - hi)[0:1], hi[1:2], (b - hi)[1:2], jnp.zeros((4, CH), jnp.float32)], axis=0)
        four = lax.dot_general(four.astype(jnp.bfloat16), order, (((1,), (1,)), ((), ())),
                               preferred_element_type=jnp.float32)
        four = jnp.concatenate([four[:, :128], four[:, 128:]], axis=0).astype(jnp.bfloat16)
        kk = jnp.dot(order, keys, preferred_element_type=jnp.float32)
        top, bottom = kk[:128], kk[128:]
        packed = (jnp.where(half, top, pltpu.roll(bottom, 64, 1)), jnp.where(half, pltpu.roll(top, 64, 1), bottom))
        vv = jnp.dot(order, values, preferred_element_type=jnp.float32).T.astype(jnp.bfloat16)
        for l in range(2):
            kvp[l, k, 0:128, :] = packed[l].astype(jnp.bfloat16)
            kvp[l, k, 128:192, :] = vv[l * 64:(l + 1) * 64, :128]
            kvp[l, k, 192:256, :] = vv[l * 64:(l + 1) * 64, 128:]
            kvp[l, k, 256:272, :] = four

    for c in local:
        c.start()
    tk[t] = tokens[...]
    pl.semaphore_wait(barrier, expected)
    for k in range(2):
        for c in feature_sends(k):
            c.start()


    def key_copy(l, k):
        g = 2 * core + l
        return remote(kvp.at[l, k], kvb.at[me, k], sk.at[l, k], rk.at[me, k], g * 4 + x, t)

    def send_keys(k):
        for l in range(2):
            @pl.when(2 * core + l != z)
            def _():
                key_copy(l, k).start()

            @pl.when(2 * core + l == z)
            def _():
                kvb[me, k] = kvp[l, k]

    def pass_on(b, k, to, sem, tp=t, src=None):
        return remote(kvb.at[b, k] if src is None else src, kvb.at[b, k], sem, rk.at[b, k], to, tp)

    def arrived(b, k):
        pass_on(b, k, me, sk.at[0, 0]).wait_recv()

    def own_column(k):
        @pl.when(active)
        def _():
            for zs in range(4):
                b = zs * 4 + x

                def spread(src):
                    pass_on(b, k, right, xk.at[zs, k, 0], src=src).start()
                    pass_on(b, k, left, xk.at[zs, k, 1], src=src).start()
                    pass_on(b, k, me, dk.at[b, k], partner, src=src).start()

                @pl.when(z != zs)
                def _():
                    arrived(b, k)
                    spread(None)

                @pl.when(z == zs)
                def _():
                    spread(kvp.at[zs % 2, k])

    def near_columns(k):
        @pl.when(active)
        def _():
            for zs in range(4):
                even = (zs + k) % 2 == 0
                b = zs * 4 + (x + 3) % 4
                arrived(b, k)
                if even:
                    pass_on(b, k, right, fk.at[zs, k]).start()
                pass_on(b, k, me, dk.at[b, k], partner).start()
                b = zs * 4 + (x + 1) % 4
                arrived(b, k)
                if not even:
                    pass_on(b, k, left, fk.at[zs, k]).start()
                pass_on(b, k, me, dk.at[b, k], partner).start()

    def far_column(k):
        @pl.when(active)
        def _():
            for zs in range(4):
                b = zs * 4 + (x + 2) % 4
                arrived(b, k)
                pass_on(b, k, me, dk.at[b, k], partner).start()

    brow = lax.broadcasted_iota(jnp.int32, (16, 256), 0)
    bcol = lax.broadcasted_iota(jnp.int32, (16, 256), 1)
    bpart = bcol % 128 - 64
    select = jnp.where((bpart >= 0) & (bpart < 2) & (brow == (bcol // 128) * 8 + 2 * (z % 2) + bpart), 1.0, 0.0)
    select = select.astype(jnp.bfloat16)

    def unpack(column):
        def chunk(k, _):
            for zs in range(4):
                b = zs * 4 + column
                packed = kvb[b, k, 0:128, :].astype(jnp.float32)
                extra = lax.dot_general(kvb[b, k, 256:272, :], select, (((0,), (0,)), ((), ())),
                                        preferred_element_type=jnp.float32)
                kx[b, k, 0:128, :] = jnp.where(half, packed, extra[:, :128]).astype(jnp.bfloat16)
                kx[b, k, 128:256, :] = jnp.where(half, pltpu.roll(packed, 64, 1), extra[:, 128:]).astype(jnp.bfloat16)
            return 0
        lax.fori_loop(0, NT, chunk, 0)

    def passive_arrivals(column):
        @pl.when(jnp.logical_not(active))
        def _():
            for k in range(NT):
                for zs in range(4):
                    arrived(zs * 4 + column, k)

    near(0)
    near(1)
    rest(0)
    for c in local[:6]:
        c.wait()
    project(0)
    send_keys(0)
    near(2)
    rest(1)
    project(1)
    send_keys(1)
    own_column(0)
    near(3)
    rest(2)
    project(2)
    send_keys(2)
    own_column(1)
    near_columns(0)
    rest(3)
    project(3)
    send_keys(3)

    def query_copy(l):
        g = 2 * core + l
        return remote(q.at[pl.ds(l * 64, 64)], qb.at[slot], sq.at[l], rq.at[slot], g * 4 + col, qtp)

    for l in range(2):
        @pl.when(query_local(l))
        def _():
            qb[slot] = q[l * 64:(l + 1) * 64, :]

    def rim_copy():
        return remote(pr.at[pl.ds(ROWS, 8)], pr.at[pl.ds(0, 8)], rim.at[0], rim.at[1], (me + 1) % 16, t)

    @pl.when(me < 15)
    def _():
        rim_copy().start()

    own_column(2)
    near_columns(1)
    far_column(0)
    own_column(3)
    near_columns(2)
    for l in range(2):
        @pl.when(jnp.logical_not(query_local(l)))
        def _():
            query_copy(l).start()
    far_column(1)


    def kchunk(c):
        return kx[c // NT, c % NT]

    def vchunk(c):
        return jnp.concatenate([kvb[c // NT, c % NT, 128:192, :], kvb[c // NT, c % NT, 192:256, :]], axis=1)

    head_rows = pl.ds(pl.multiple_of((4 * y + z) * 64, 64), 64)

    def piece_copy(s, blk, p):
        return remote(out_local.at[s, :, pl.ds(p * 128, 128)], at.at[head_rows], so.at[s, p],
                      ro.at[4 * y + z], blk, p)

    def rem_copy(s, blk):
        return remote(carry_out.at[s], rb.at[z % 2], sr.at[s], rr.at[z % 2], blk, back)

    def first_part(s):
        blk = set_block(x, core, s)

        @pl.when(jnp.logical_not((blk == me) & (core == z // 2)))
        def _():
            remote(qb.at[s], qb.at[s], sq.at[0], rq.at[s], me, t).wait_recv()
        qs = qb[s].astype(jnp.float32) * (HEAD_DIM ** -0.5 * LOG2E)
        hi = qs.astype(jnp.bfloat16)
        qt[s, 0:64] = hi
        qt[s, 64:128] = jnp.where(lax.broadcasted_iota(jnp.int32, (64, ROWS), 0) < 2, 1.0, 0.0).astype(jnp.bfloat16)
        qt[s, 128:192] = (qs - hi.astype(jnp.float32)).astype(jnp.bfloat16)
        qt[s, 192:256] = jnp.zeros((64, ROWS), jnp.bfloat16)
        attend_own(qt.at[s], blk, kchunk, vchunk, sums.at[s], carry.at[s], ya, wb.at[s])

    near_columns(3)
    @pl.when(me == 0)
    def _():
        pr[0:8, :] = jnp.zeros((8, 128), jnp.float32)

    @pl.when(me > 0)
    def _():
        rim_copy().wait_recv()
    tp_values = taps[...].astype(jnp.float32)
    running = jnp.zeros((ROWS, 128), jnp.float32)
    for w in range(CONV_W):
        running = running + tp_values[w:w + 1, :] * pr[6 + w:6 + w + ROWS, :]
    fl[...] = (post[...].astype(jnp.float32) * running).astype(jnp.bfloat16)

    @pl.when(me < 15)
    def _():
        rim_copy().wait_send()

    def lanes(i):
        return pl.ds(pl.multiple_of(i * 128, 128), 128)

    def filter_copy(n):
        p = (t + n) % 8
        return remote(fl.at[lanes(p)], fa.at[:, lanes(t)], sf.at[n], sf.at[8 + n], me, p)

    for n in range(1, 8):
        filter_copy(n).start()
    fa[:, lanes(t)] = fl[lanes(t), :]
    for c in (0, 3, 1):
        passive_arrivals((x + c) % 4)
        unpack((x + c) % 4)
    far_column(2)
    first_part(1)
    far_column(3)
    first_part(0)
    passive_arrivals((x + 2) % 4)
    unpack((x + 2) % 4)

    for s in range(2):
        blk = set_block(x, core, s)
        own = (blk == me) & (core == z // 2)
        attend_before(qt.at[s], blk, kchunk, vchunk, sums.at[s], carry.at[s], ya, yb, wa, wb.at[s])
        for i in range(NT):
            out_local[s, :, i * CH:(i + 1) * CH] = sums[s, i].astype(jnp.bfloat16)
            carry_out[s, :, i * CH:(i + 1) * CH] = carry[s, i]
        for p in range(8):
            here = (blk == me) & (t == p)

            @pl.when(jnp.logical_not(here))
            def _():
                piece_copy(s, blk, p).start()

            @pl.when(here)
            def _():
                at[head_rows, :] = out_local[s, :, p * 128:(p + 1) * 128]

        @pl.when(jnp.logical_not(own))
        def _():
            rem_copy(s, blk).start()

        @pl.when(own)
        def _():
            rb[z % 2] = carry_out[s]

        if s == 0:
            for n in range(1, 8):
                remote(fl.at[lanes(0)], fa.at[:, lanes((t - n + 8) % 8)], sf.at[n], sf.at[8 + n], me, t).wait_recv()
            local[6].wait()
            local[7].wait()
            for n in range(8):
                c = slice(n * 256, (n + 1) * 256)
                total[:, c] = jnp.dot(fa[...], fr[:, c], preferred_element_type=jnp.float32)


    for h in range(16):
        hz = h % 4
        column, hcore, _ = query_place(z, x)
        mine = (hz == z) & (column == x) & (2 * (h // 4) + hcore == t)

        @pl.when(jnp.logical_not(mine))
        def _():
            part = at.at[pl.ds(h * 64, 64)]
            remote(part, part, so.at[0, 0], ro.at[h], me, t).wait_recv()
    rows_t = at[...].astype(jnp.float32).T.astype(jnp.bfloat16)
    for n in range(8):
        c = slice(n * 256, (n + 1) * 256)
        mixed[:, c] = (total[:, c] + jnp.dot(rows_t, ar[:, c], preferred_element_type=jnp.float32)).astype(jnp.bfloat16)
    for l in range(2):
        @pl.when(jnp.logical_not(query_local(l)))
        def _():
            remote(rb.at[l], rb.at[l], sr.at[0], rr.at[l], me, t).wait_recv()
        mass[l:l + 1, :] = rb[l, 0:1, :]

    for k in range(NT):
        for c in feature_sends(k):
            c.wait_send()
        relay(k).wait_send()
        for n, sl in enumerate((down, up, far)):
            over(k, n, sl).wait_send()
    for n in range(1, 8):
        filter_copy(n).wait_send()
    for l in range(2):
        @pl.when(2 * core + l != z)
        def _():
            for k in range(NT):
                key_copy(l, k).wait_send()

        @pl.when(jnp.logical_not(query_local(l)))
        def _():
            query_copy(l).wait_send()

    @pl.when(active)
    def _():
        for k in range(NT):
            for zs in range(4):
                pass_on(zs * 4 + x, k, right, xk.at[zs, k, 0]).wait_send()
                pass_on(zs * 4 + x, k, left, xk.at[zs, k, 1]).wait_send()
                pass_on(zs * 4 + x, k, right, fk.at[zs, k]).wait_send()
            for b in range(16):
                pass_on(b, k, me, dk.at[b, k], partner).wait_send()

    for s in range(2):
        blk = set_block(x, core, s)
        own = (blk == me) & (core == z // 2)
        for p in range(8):
            @pl.when(jnp.logical_not((blk == me) & (t == p)))
            def _():
                piece_copy(s, blk, p).wait_send()

        @pl.when(jnp.logical_not(own))
        def _():
            rem_copy(s, blk).wait_send()


def per_device(tokens, norm_gain, signal_proj, postgate_proj, pregate_proj, query_proj, key_proj,
               value_proj, filter_taps, break_bias, filter_readout, attention_readout):
    vmem = pl.BlockSpec(memory_space=pltpu.VMEM)
    hbm = pl.BlockSpec(memory_space=pl.ANY)
    dma = pltpu.SemaphoreType.DMA
    bf16, f32 = jnp.bfloat16, jnp.float32
    mixed, remain = pl.pallas_call(
        layer_kernel,
        out_shape=(jax.ShapeDtypeStruct((128, 2048), bf16), jax.ShapeDtypeStruct((2, ROWS), f32)),
        in_specs=[vmem, vmem] + [hbm] * 6 + [vmem, vmem, hbm, hbm],
        out_specs=(vmem, vmem),
        scratch_shapes=[
            pltpu.VMEM((8, ROWS, 256), bf16),
            pltpu.VMEM((2048, 768), bf16),
            pltpu.VMEM((1024, 2048), bf16),
            pltpu.VMEM((1024, 2048), bf16),
            pltpu.VMEM((CH, 2048), bf16),
            pltpu.VMEM((ROWS + 8, 128), f32),
            pltpu.VMEM((ROWS, 128), bf16),
            pltpu.VMEM((ROWS, 128), bf16),
            pltpu.VMEM((128, ROWS), bf16),
            pltpu.VMEM((2, NT, 272, 128), bf16),
            pltpu.VMEM((16, NT, 272, 128), bf16),
            pltpu.VMEM((16, NT, CH, 128), bf16),
            pltpu.VMEM((2, 64, ROWS), bf16),
            pltpu.VMEM((2, 8, ROWS), f32),
            pltpu.VMEM((128, 1024), bf16),
            pltpu.VMEM((1024, 128), bf16),
            pltpu.VMEM((128, 2048), f32),
            pltpu.VMEM((2, 256, ROWS), bf16),
            pltpu.VMEM((2, 64, ROWS), bf16),
            pltpu.VMEM((2, 8, ROWS), f32),
            pltpu.VMEM((2, NT, 64, CH), f32),
            pltpu.VMEM((2, NT, 8, CH), f32),
            pltpu.VMEM((NT, CH, CH), f32),
            pltpu.VMEM((NT, CH, CH), f32),
            pltpu.VMEM((NT, CH, CH), bf16),
            pltpu.VMEM((2, NT, CH, CH), bf16),
            dma((8,)), dma((4, 8)), dma((8, 4)), dma((16,)), dma((2,)),
            dma((16, 4)), dma((2,)), dma((16,)), dma((2,)),
            dma((2, 4)), dma((2,)), dma((2, 8)), dma((2,)),
            dma((4, 4, 2)), dma((16, 4)), dma((4, 4)),
        ],
        compiler_params=pltpu.CompilerParams(vmem_limit_bytes=60 * 2**20, has_side_effects=True, collective_id=0),
    )(tokens, norm_gain.reshape(1, -1), signal_proj, postgate_proj, pregate_proj, query_proj, key_proj,
      value_proj, filter_taps, break_bias.T, filter_readout, attention_readout)
    return mixed, jnp.log(jnp.maximum(1.0 - remain, mass_floor))


def solution(mesh):
    placed = (P("sp", "tp"), P()) + (P(None, "tp"),) * 7 + (P("sp", "tp"), P(), P())
    return jax.shard_map(per_device, mesh=mesh, in_specs=placed,
                         out_specs=(P(("sp", "tp"), None), P("tp", "sp")), check_vma=False)
```

```python
import jax
import jax.numpy as jnp
from jax import lax
from jax.experimental import pallas as pl
from jax.experimental.pallas import tpu as pltpu
from jax.sharding import PartitionSpec as P

HEAD_DIM = 64
CONV_W = 3
CH = 256
NT = 4
CAP = 24.0
QROWS = 256
LOG2E = 1.4426950408889634
epsilon = 1e-06
mass_floor = 0.1


def scan_chunk(y_ref, carry_ref, w_ref, masked):
    seg = CH // 8
    if masked:
        row = lax.broadcasted_iota(jnp.int32, (8, CH), 0) * seg
        col = lax.broadcasted_iota(jnp.int32, (8, CH), 1)
        diff = col - row
    r = jnp.ones((8, CH), jnp.float32)
    for g in reversed(range(seg // 4)):
        us, ds = [], []
        for k in range(4):
            j = 4 * g + k
            u = jnp.exp2(jnp.minimum(y_ref[j * 8:(j + 1) * 8, :], CAP))
            if masked:
                u = jnp.where(diff > j, u, 0.0)
            us.append(u)
            ds.append(1.0 + u)
        low, high = ds[0] * ds[1], ds[2] * ds[3]
        r = r * (1.0 / (low * high))
        e = r * low
        ws = [us[0] * r, us[1] * (r * ds[0]), us[2] * e, us[3] * (e * ds[2])]
        for k in (0, 2):
            j = 4 * g + k
            w_ref[j * 8:(j + 2) * 8, :] = jnp.concatenate(ws[k:k + 2], axis=0).astype(jnp.bfloat16)
    sub = lax.broadcasted_iota(jnp.int32, (8, CH), 0)
    s = r
    for k in (1, 2, 4):
        s = s * jnp.where(sub < 8 - k, pltpu.roll(s, 8 - k, 0), 1.0)
    carry = carry_ref[...]
    c = jnp.where(sub < 7, pltpu.roll(s, 7, 0), 1.0) * carry
    carry_ref[...] = carry * jnp.broadcast_to(s[0:1, :], (8, CH))
    c = jnp.concatenate([c, c], axis=0).astype(jnp.bfloat16)
    for j in range(CH // 16):
        w_ref[j * 16:(j + 1) * 16, :] = w_ref[j * 16:(j + 1) * 16, :] * c

def scores_to(y_ref, kk, q_ref, tile):
    lhs = jnp.concatenate([kk, kk], axis=1)
    rhs = q_ref[:, tile * CH:(tile + 1) * CH]
    for i in range(0, CH, QROWS):
        y_ref[i:i + QROWS, :] = jnp.dot(lhs[i:i + QROWS], rhs, preferred_element_type=jnp.float32)

def attend_own(qt, blk, kchunk, vchunk, acc, carry, ya, wb):
    base = 4 * blk
    for t in range(NT):
        acc[t] = jnp.zeros_like(acc[t])
        carry[t] = jnp.ones((8, CH), jnp.float32)
    for c in reversed(range(NT)):
        kk = kchunk(base + c)
        for t in range(c, NT):
            scores_to(ya.at[t], kk, qt, t)
        for t in range(c, NT):
            scan_chunk(ya.at[t], carry.at[t], wb.at[t], t == c)
        if c > 0:
            vv = vchunk(base + c)
            for t in range(c, NT):
                acc[t] += jnp.dot(vv, wb[t], preferred_element_type=jnp.float32)


def attend_before(qt, blk, kchunk, vchunk, acc, carry, ya, yb, wa, wb):
    base = 4 * blk
    kk = kchunk(jnp.maximum(base - 1, 0))
    for t in range(NT):
        scores_to(ya.at[t], kk, qt, t)

    def half(c, ysrc, ydst, wdst, wsrc):
        kn = kchunk(jnp.maximum(c - 1, 0))
        vp = vchunk(c + 1)
        for t in range(NT):
            scan_chunk(ysrc.at[t], carry.at[t], wdst.at[t], False)
            scores_to(ydst.at[t], kn, qt, t)
            acc[t] += jnp.dot(vp, wsrc[t], preferred_element_type=jnp.float32)

    def body(p, _):
        c = base - 1 - 2 * p
        half(c, ya, yb, wa, wb)
        half(c - 1, yb, ya, wb, wa)
        return 0
    lax.fori_loop(0, 2 * blk, body, 0)
    vp = vchunk(0)
    for t in range(NT):
        acc[t] += jnp.dot(vp, wb[t], preferred_element_type=jnp.float32)


SP, TP = "sp", "tp"
ROWS = NT * CH


def remote(src, dst, send, recv, sp, tp):
    return pltpu.make_async_remote_copy(src_ref=src, dst_ref=dst, send_sem=send, recv_sem=recv,
                                        device_id={SP: sp, TP: tp}, device_id_type=pl.DeviceIdType.MESH)


def query_place(z, x):
    column = jnp.where((z == 1) | (z == 3), 3 - x, x)
    core = jnp.where((z == 1) | (z == 2), 1, 0)
    slot = jnp.where((z == 2) | (z == 3), 0, 1)
    return column, core, slot


def set_block(x, core, slot):
    return jnp.where(core == 0, jnp.where(slot == 0, 15 - x, x), jnp.where(slot == 0, 8 + x, 7 - x))


def layer_kernel(tokens, gain, w0, w1, w2, w3, w4, w5, taps, bias, fr_hbm, ar_hbm, mixed, mass,
                 tk, wts, fr, ar, sc, pr, post, fl, q, kvp, kvb, kx, qb, rb, fa, at, total,
                 qt, out_local, carry_out, sums, carry, ya, yb, wa, wb,
                 lw, st, rt, sf, rim,
                 rk, rq, ro, rr, sk, sq, so, sr, xk, dk, fk):
    me = lax.axis_index(SP)
    t = lax.axis_index(TP)
    z, x = me // 4, me % 4
    core = t % 2
    y = t // 2
    partner = t + 1 - 2 * core
    active = core == z // 2
    right = z * 4 + (x + 1) % 4
    left = z * 4 + (x + 3) % 4

    back = t - core + z // 2
    col, qcore, slot = query_place(z, x)
    qtp = t - core + qcore

    def query_local(l):
        return (2 * core + l == z) & (col == x) & (qcore == core)

    barrier = pltpu.get_barrier_semaphore()

    def greet(sp, tp):
        pl.semaphore_signal(barrier, inc=1, device_id={SP: sp, TP: tp}, device_id_type=pl.DeviceIdType.MESH)

    for n in range(1, 8):
        greet(me, (t + n) % 8)
    greet(right, t)
    greet(left, t)
    for n in range(1, 4):
        greet((me + 4 * n) % 16, t)
    expected = 12
    for s in range(2):
        blk = set_block(x, core, s)

        @pl.when(jnp.logical_not((blk == me) & (core == z // 2)))
        def _():
            greet(blk, back)
        expected = expected + jnp.where(query_local(s), 0, 1)

    @pl.when(me > 0)
    def _():
        greet(me - 1, t)
    expected = expected + jnp.where(me < 15, 1, 0)

    local = [pltpu.make_async_copy(w, wts.at[:, i * 128:(i + 1) * 128], lw.at[i])
             for i, w in enumerate((w0, w1, w2, w3, w4, w5))]
    local += [pltpu.make_async_copy(fr_hbm, fr, lw.at[6]), pltpu.make_async_copy(ar_hbm, ar, lw.at[7])]

    up = (t + 2) % 8
    down = (t + 6) % 8
    far = (t + 4) % 8

    def rows(k):
        return pl.ds(k * CH, CH)

    def feature_sends(k):
        src = tokens.at[rows(k)]
        dst = tk.at[t, rows(k)]
        return [remote(src, dst, st.at[k, 0], rt.at[t, k], me, up),
                remote(src, dst, st.at[k, 1], rt.at[t, k], me, down),
                remote(src, dst, st.at[k, 2], rt.at[t, k], me, partner)]

    def relay(k):
        slot, to = (down, up) if k % 2 == 0 else (up, down)
        part = tk.at[slot, rows(k)]
        return remote(part, part, st.at[k, 3], rt.at[slot, k], me, to)

    def over(k, n, slot):
        part = tk.at[slot, rows(k)]
        return remote(part, part, st.at[k, 4 + n], rt.at[slot, k], me, partner)

    def got(slot, k):
        part = tk.at[slot, rows(k)]
        remote(part, part, st.at[k, 0], rt.at[slot, k], me, t).wait_recv()

    def near(k):
        got(down, k)
        got(up, k)
        relay(k).start()
        over(k, 0, down).start()
        over(k, 1, up).start()
        if k + 2 < NT:
            for c in feature_sends(k + 2):
                c.start()

    def rest(k):
        got(far, k)
        over(k, 2, far).start()
        for n in (0, 2, 4, 6):
            got((partner + n) % 8, k)

    rowi = lax.broadcasted_iota(jnp.int32, (CH, CH), 0)
    coli = lax.broadcasted_iota(jnp.int32, (CH, CH), 1)
    order = jnp.where(coli == (rowi % 8) * (CH // 8) + rowi // 8, 1.0, 0.0).astype(jnp.bfloat16)
    half = lax.broadcasted_iota(jnp.int32, (128, 128), 1) < 64

    def project(k):
        r = rows(k)
        squares = jnp.zeros((CH, 128), jnp.float32)
        for s in range(8):
            v = tk[s, r, :].astype(jnp.float32)
            v2 = v * v
            squares = squares + v2[:, :128] + v2[:, 128:]
            sc[:, s * 256:(s + 1) * 256] = (v * gain[:, s * 256:(s + 1) * 256]).astype(jnp.bfloat16)
        inverse = lax.rsqrt(jnp.sum(squares, axis=1, keepdims=True) * (1.0 / 2048.0) + epsilon)

        def product(n):
            p = jnp.dot(sc[...], wts[:, n * 256:(n + 1) * 256], preferred_element_type=jnp.float32)
            p = (p * inverse).astype(jnp.bfloat16)
            return p[:, :128], p[:, 128:]

        signal, post_gate = product(0)
        pre_gate, queries = product(1)
        keys, values = product(2)
        pr[8 + k * CH:8 + (k + 1) * CH, :] = pre_gate.astype(jnp.float32) * signal.astype(jnp.float32)
        post[r, :] = post_gate
        q[:, r] = queries.astype(jnp.float32).T.astype(jnp.bfloat16)
        b = bias[:, r].astype(jnp.float32) * LOG2E
        hi = b.astype(jnp.bfloat16).astype(jnp.float32)
        four = jnp.concatenate([hi[0:1], (b - hi)[0:1], hi[1:2], (b - hi)[1:2], jnp.zeros((4, CH), jnp.float32)], axis=0)
        four = lax.dot_general(four.astype(jnp.bfloat16), order, (((1,), (1,)), ((), ())),
                               preferred_element_type=jnp.float32)
        four = jnp.concatenate([four[:, :128], four[:, 128:]], axis=0).astype(jnp.bfloat16)
        kk = jnp.dot(order, keys, preferred_element_type=jnp.float32)
        top, bottom = kk[:128], kk[128:]
        packed = (jnp.where(half, top, pltpu.roll(bottom, 64, 1)), jnp.where(half, pltpu.roll(top, 64, 1), bottom))
        vv = jnp.dot(order, values, preferred_element_type=jnp.float32).T.astype(jnp.bfloat16)
        for l in range(2):
            kvp[l, k, 0:128, :] = packed[l].astype(jnp.bfloat16)
            kvp[l, k, 128:192, :] = vv[l * 64:(l + 1) * 64, :128]
            kvp[l, k, 192:256, :] = vv[l * 64:(l + 1) * 64, 128:]
            kvp[l, k, 256:272, :] = four

    for c in local:
        c.start()
    tk[t] = tokens[...]
    pl.semaphore_wait(barrier, expected)
    for k in range(2):
        for c in feature_sends(k):
            c.start()


    def key_copy(l, k):
        g = 2 * core + l
        return remote(kvp.at[l, k], kvb.at[me, k], sk.at[l, k], rk.at[me, k], g * 4 + x, t)

    def send_keys(k):
        for l in range(2):
            @pl.when(2 * core + l != z)
            def _():
                key_copy(l, k).start()

            @pl.when(2 * core + l == z)
            def _():
                kvb[me, k] = kvp[l, k]

    def pass_on(b, k, to, sem, tp=t, src=None):
        return remote(kvb.at[b, k] if src is None else src, kvb.at[b, k], sem, rk.at[b, k], to, tp)

    def arrived(b, k):
        pass_on(b, k, me, sk.at[0, 0]).wait_recv()

    def own_column(k):
        @pl.when(active)
        def _():
            for zs in range(4):
                b = zs * 4 + x

                def spread(src):
                    pass_on(b, k, right, xk.at[zs, k, 0], src=src).start()
                    pass_on(b, k, left, xk.at[zs, k, 1], src=src).start()
                    pass_on(b, k, me, dk.at[b, k], partner, src=src).start()

                @pl.when(z != zs)
                def _():
                    arrived(b, k)
                    spread(None)

                @pl.when(z == zs)
                def _():
                    spread(kvp.at[zs % 2, k])

    def near_columns(k):
        @pl.when(active)
        def _():
            for zs in range(4):
                even = (zs + k) % 2 == 0
                b = zs * 4 + (x + 3) % 4
                arrived(b, k)
                if even:
                    pass_on(b, k, right, fk.at[zs, k]).start()
                pass_on(b, k, me, dk.at[b, k], partner).start()
                b = zs * 4 + (x + 1) % 4
                arrived(b, k)
                if not even:
                    pass_on(b, k, left, fk.at[zs, k]).start()
                pass_on(b, k, me, dk.at[b, k], partner).start()

    def far_column(k):
        @pl.when(active)
        def _():
            for zs in range(4):
                b = zs * 4 + (x + 2) % 4
                arrived(b, k)
                pass_on(b, k, me, dk.at[b, k], partner).start()

    brow = lax.broadcasted_iota(jnp.int32, (16, 256), 0)
    bcol = lax.broadcasted_iota(jnp.int32, (16, 256), 1)
    bpart = bcol % 128 - 64
    select = jnp.where((bpart >= 0) & (bpart < 2) & (brow == (bcol // 128) * 8 + 2 * (z % 2) + bpart), 1.0, 0.0)
    select = select.astype(jnp.bfloat16)

    def unpack(column):
        def chunk(k, _):
            for zs in range(4):
                b = zs * 4 + column
                packed = kvb[b, k, 0:128, :].astype(jnp.float32)
                extra = lax.dot_general(kvb[b, k, 256:272, :], select, (((0,), (0,)), ((), ())),
                                        preferred_element_type=jnp.float32)
                kx[b, k, 0:128, :] = jnp.where(half, packed, extra[:, :128]).astype(jnp.bfloat16)
                kx[b, k, 128:256, :] = jnp.where(half, pltpu.roll(packed, 64, 1), extra[:, 128:]).astype(jnp.bfloat16)
            return 0
        lax.fori_loop(0, NT, chunk, 0)

    def passive_arrivals(column):
        @pl.when(jnp.logical_not(active))
        def _():
            for k in range(NT):
                for zs in range(4):
                    arrived(zs * 4 + column, k)

    near(0)
    near(1)
    rest(0)
    for c in local[:6]:
        c.wait()
    project(0)
    send_keys(0)
    near(2)
    rest(1)
    project(1)
    send_keys(1)
    own_column(0)
    near(3)
    rest(2)
    project(2)
    send_keys(2)
    own_column(1)
    near_columns(0)
    rest(3)
    project(3)
    send_keys(3)

    def query_copy(l):
        g = 2 * core + l
        return remote(q.at[pl.ds(l * 64, 64)], qb.at[slot], sq.at[l], rq.at[slot], g * 4 + col, qtp)

    for l in range(2):
        @pl.when(query_local(l))
        def _():
            qb[slot] = q[l * 64:(l + 1) * 64, :]

    def rim_copy():
        return remote(pr.at[pl.ds(ROWS, 8)], pr.at[pl.ds(0, 8)], rim.at[0], rim.at[1], (me + 1) % 16, t)

    @pl.when(me < 15)
    def _():
        rim_copy().start()

    own_column(2)
    near_columns(1)
    far_column(0)
    own_column(3)
    near_columns(2)
    for l in range(2):
        @pl.when(jnp.logical_not(query_local(l)))
        def _():
            query_copy(l).start()
    far_column(1)


    def kchunk(c):
        return kx[c // NT, c % NT]

    def vchunk(c):
        return jnp.concatenate([kvb[c // NT, c % NT, 128:192, :], kvb[c // NT, c % NT, 192:256, :]], axis=1)

    head_rows = pl.ds(pl.multiple_of((4 * y + z) * 64, 64), 64)

    def piece_copy(s, blk, n):
        p = (t + n) % 8
        return remote(out_local.at[s, :, lanes(p)], at.at[head_rows], so.at[s, n],
                      ro.at[4 * y + z], blk, p)

    def rem_copy(s, blk):
        return remote(carry_out.at[s], rb.at[z % 2], sr.at[s], rr.at[z % 2], blk, back)

    def first_part(s):
        blk = set_block(x, core, s)

        @pl.when(jnp.logical_not((blk == me) & (core == z // 2)))
        def _():
            remote(qb.at[s], qb.at[s], sq.at[0], rq.at[s], me, t).wait_recv()
        qs = qb[s].astype(jnp.float32) * (HEAD_DIM ** -0.5 * LOG2E)
        hi = qs.astype(jnp.bfloat16)
        qt[s, 0:64] = hi
        qt[s, 64:128] = jnp.where(lax.broadcasted_iota(jnp.int32, (64, ROWS), 0) < 2, 1.0, 0.0).astype(jnp.bfloat16)
        qt[s, 128:192] = (qs - hi.astype(jnp.float32)).astype(jnp.bfloat16)
        qt[s, 192:256] = jnp.zeros((64, ROWS), jnp.bfloat16)
        attend_own(qt.at[s], blk, kchunk, vchunk, sums.at[s], carry.at[s], ya, wb.at[s])

    near_columns(3)
    @pl.when(me == 0)
    def _():
        pr[0:8, :] = jnp.zeros((8, 128), jnp.float32)

    @pl.when(me > 0)
    def _():
        rim_copy().wait_recv()
    tp_values = taps[...].astype(jnp.float32)
    running = jnp.zeros((ROWS, 128), jnp.float32)
    for w in range(CONV_W):
        running = running + tp_values[w:w + 1, :] * pr[6 + w:6 + w + ROWS, :]
    fl[...] = (post[...].astype(jnp.float32) * running).astype(jnp.bfloat16)

    @pl.when(me < 15)
    def _():
        rim_copy().wait_send()

    def lanes(i):
        return pl.ds(pl.multiple_of(i * 128, 128), 128)

    def filter_copy(n):
        p = (t + n) % 8
        return remote(fl.at[lanes(p)], fa.at[:, lanes(t)], sf.at[n], sf.at[8 + n], me, p)

    for n in range(1, 8):
        filter_copy(n).start()
    fa[:, lanes(t)] = fl[lanes(t), :]
    for c in (0, 3, 1):
        passive_arrivals((x + c) % 4)
        unpack((x + c) % 4)
    far_column(2)
    first_part(1)
    far_column(3)
    first_part(0)
    passive_arrivals((x + 2) % 4)
    unpack((x + 2) % 4)

    for s in range(2):
        blk = set_block(x, core, s)
        own = (blk == me) & (core == z // 2)
        attend_before(qt.at[s], blk, kchunk, vchunk, sums.at[s], carry.at[s], ya, yb, wa, wb.at[s])
        for i in range(NT):
            out_local[s, :, i * CH:(i + 1) * CH] = sums[s, i].astype(jnp.bfloat16)
            carry_out[s, :, i * CH:(i + 1) * CH] = carry[s, i]
        for p in range(8):
            here = (blk == me) & (p == 0)

            @pl.when(jnp.logical_not(here))
            def _():
                piece_copy(s, blk, p).start()

            @pl.when(here)
            def _():
                at[head_rows, :] = out_local[s, :, lanes((t + p) % 8)]

        @pl.when(jnp.logical_not(own))
        def _():
            rem_copy(s, blk).start()

        @pl.when(own)
        def _():
            rb[z % 2] = carry_out[s]

        if s == 0:
            for n in range(1, 8):
                remote(fl.at[lanes(0)], fa.at[:, lanes((t - n + 8) % 8)], sf.at[n], sf.at[8 + n], me, t).wait_recv()
            local[6].wait()
            local[7].wait()
            for n in range(8):
                c = slice(n * 256, (n + 1) * 256)
                total[:, c] = jnp.dot(fa[...], fr[:, c], preferred_element_type=jnp.float32)


    for h in range(16):
        hz = h % 4
        column, hcore, _ = query_place(z, x)
        mine = (hz == z) & (column == x) & (2 * (h // 4) + hcore == t)

        @pl.when(jnp.logical_not(mine))
        def _():
            part = at.at[pl.ds(h * 64, 64)]
            remote(part, part, so.at[0, 0], ro.at[h], me, t).wait_recv()
    rows_t = at[...].astype(jnp.float32).T.astype(jnp.bfloat16)
    for n in range(8):
        c = slice(n * 256, (n + 1) * 256)
        mixed[:, c] = (total[:, c] + jnp.dot(rows_t, ar[:, c], preferred_element_type=jnp.float32)).astype(jnp.bfloat16)
    for l in range(2):
        @pl.when(jnp.logical_not(query_local(l)))
        def _():
            remote(rb.at[l], rb.at[l], sr.at[0], rr.at[l], me, t).wait_recv()
        mass[l:l + 1, :] = rb[l, 0:1, :]

    for k in range(NT):
        for c in feature_sends(k):
            c.wait_send()
        relay(k).wait_send()
        for n, sl in enumerate((down, up, far)):
            over(k, n, sl).wait_send()
    for n in range(1, 8):
        filter_copy(n).wait_send()
    for l in range(2):
        @pl.when(2 * core + l != z)
        def _():
            for k in range(NT):
                key_copy(l, k).wait_send()

        @pl.when(jnp.logical_not(query_local(l)))
        def _():
            query_copy(l).wait_send()

    @pl.when(active)
    def _():
        for k in range(NT):
            for zs in range(4):
                pass_on(zs * 4 + x, k, right, xk.at[zs, k, 0]).wait_send()
                pass_on(zs * 4 + x, k, left, xk.at[zs, k, 1]).wait_send()
                pass_on(zs * 4 + x, k, right, fk.at[zs, k]).wait_send()
            for b in range(16):
                pass_on(b, k, me, dk.at[b, k], partner).wait_send()

    for s in range(2):
        blk = set_block(x, core, s)
        own = (blk == me) & (core == z // 2)
        for p in range(8):
            @pl.when(jnp.logical_not((blk == me) & (p == 0)))
            def _():
                piece_copy(s, blk, p).wait_send()

        @pl.when(jnp.logical_not(own))
        def _():
            rem_copy(s, blk).wait_send()


def per_device(tokens, norm_gain, signal_proj, postgate_proj, pregate_proj, query_proj, key_proj,
               value_proj, filter_taps, break_bias, filter_readout, attention_readout):
    vmem = pl.BlockSpec(memory_space=pltpu.VMEM)
    hbm = pl.BlockSpec(memory_space=pl.ANY)
    dma = pltpu.SemaphoreType.DMA
    bf16, f32 = jnp.bfloat16, jnp.float32
    mixed, remain = pl.pallas_call(
        layer_kernel,
        out_shape=(jax.ShapeDtypeStruct((128, 2048), bf16), jax.ShapeDtypeStruct((2, ROWS), f32)),
        in_specs=[vmem, vmem] + [hbm] * 6 + [vmem, vmem, hbm, hbm],
        out_specs=(vmem, vmem),
        scratch_shapes=[
            pltpu.VMEM((8, ROWS, 256), bf16),
            pltpu.VMEM((2048, 768), bf16),
            pltpu.VMEM((1024, 2048), bf16),
            pltpu.VMEM((1024, 2048), bf16),
            pltpu.VMEM((CH, 2048), bf16),
            pltpu.VMEM((ROWS + 8, 128), f32),
            pltpu.VMEM((ROWS, 128), bf16),
            pltpu.VMEM((ROWS, 128), bf16),
            pltpu.VMEM((128, ROWS), bf16),
            pltpu.VMEM((2, NT, 272, 128), bf16),
            pltpu.VMEM((16, NT, 272, 128), bf16),
            pltpu.VMEM((16, NT, CH, 128), bf16),
            pltpu.VMEM((2, 64, ROWS), bf16),
            pltpu.VMEM((2, 8, ROWS), f32),
            pltpu.VMEM((128, 1024), bf16),
            pltpu.VMEM((1024, 128), bf16),
            pltpu.VMEM((128, 2048), f32),
            pltpu.VMEM((2, 256, ROWS), bf16),
            pltpu.VMEM((2, 64, ROWS), bf16),
            pltpu.VMEM((2, 8, ROWS), f32),
            pltpu.VMEM((2, NT, 64, CH), f32),
            pltpu.VMEM((2, NT, 8, CH), f32),
            pltpu.VMEM((NT, CH, CH), f32),
            pltpu.VMEM((NT, CH, CH), f32),
            pltpu.VMEM((NT, CH, CH), bf16),
            pltpu.VMEM((2, NT, CH, CH), bf16),
            dma((8,)), dma((4, 8)), dma((8, 4)), dma((16,)), dma((2,)),
            dma((16, 4)), dma((2,)), dma((16,)), dma((2,)),
            dma((2, 4)), dma((2,)), dma((2, 8)), dma((2,)),
            dma((4, 4, 2)), dma((16, 4)), dma((4, 4)),
        ],
        compiler_params=pltpu.CompilerParams(vmem_limit_bytes=60 * 2**20, has_side_effects=True, collective_id=0),
    )(tokens, norm_gain.reshape(1, -1), signal_proj, postgate_proj, pregate_proj, query_proj, key_proj,
      value_proj, filter_taps, break_bias.T, filter_readout, attention_readout)
    return mixed, jnp.log(jnp.maximum(1.0 - remain, mass_floor))


def solution(mesh):
    placed = (P("sp", "tp"), P()) + (P(None, "tp"),) * 7 + (P("sp", "tp"), P(), P())
    return jax.shard_map(per_device, mesh=mesh, in_specs=placed,
                         out_specs=(P(("sp", "tp"), None), P("tp", "sp")), check_vma=False)
```
